256 devices in a mesh: ep: 64 (over z, y, core), tp: 4 (over x).
Axes of the slice: x: 4, y: 4, z: 8, core: 2. Of those that a mesh axis runs over, the one named last changes fastest.
Arguments:
- tokens: bfloat16 [3072, 2048], P('ep'), may hold values from -6 to 6
- out_grad: bfloat16 [3072, 2048], P('ep'), may hold values from -4 to 4
- expert_ids: int32 [3072, 4], P('ep'), may hold values from 0 to 63, all different within a row; in each aligned block of 48 rows (0 to 47, 48 to 95, ...) at most 8 rows name the same one
- router_weight: bfloat16 [2048, 64], replicated, may hold values from -0.125 to 0.125
- w_gate: bfloat16 [64, 2048, 1536], P('ep', None, 'tp'), may hold values from -0.125 to 0.125
- w_up: bfloat16 [64, 2048, 1536], P('ep', None, 'tp'), may hold values from -0.125 to 0.125
- w_down: bfloat16 [64, 1536, 2048], P('ep', 'tp'), may hold values from -0.15625 to 0.15625
Outputs:
- token_grad: bfloat16 [3072, 2048], P('ep', 'tp')
- router_grad: float32 [2048, 64], P('tp', 'ep')
- w_gate_grad: bfloat16 [64, 2048, 1536], P('ep', None, 'tp')
- w_up_grad: bfloat16 [64, 2048, 1536], P('ep', None, 'tp')
- w_down_grad: bfloat16 [64, 1536, 2048], P('ep', 'tp')
The draws below stay inside these ranges and needn't reach their ends.
Inputs may be any that keep to these rules, and one draw needn't show every extreme that they name: `expert_ids`: each row names 4 different experts; among the rows of one device no expert is named more than 8 times, and in some devices' rows one expert is named exactly 8 times.
All inputs are finite; a program needn't handle non-finite values.
Results may differ from the reference program's by a relative error of at most 0.0058.
Values may be sent and summed in bfloat16 or wider, within the bound.
No kernel may reach another device: no remote copies, remote signals or barrier semaphores. Data moves between devices by JAX's collectives and lax.ppermute only.
A program may use at most 128 MiB of HBM per device.

```python
import math
import jax
import jax.numpy as jnp
import numpy as np
from jax import lax

D = 2048
FF = 1536
TOPK = 4
TOK_DEV = 48
EXPERTS = 64
TOKENS = 3072
CAP = 8
N_EP = 64


def draw_tokens(key, part):
    base_key = jax.random.fold_in(key, 11)
    pick_key = jax.random.fold_in(key, 12)
    base = jax.random.normal(base_key, (TOKENS, D), jnp.float32)
    strong = jax.random.randint(pick_key, (TOKENS, 1), 0, 16) == 0
    values = jnp.where(strong, 4.0 * base, base)
    return jnp.clip(values, -6.0, 6.0).astype(jnp.bfloat16)


def shard_levels(stream_key, shape, pieces, least, high):
    def one(dim, parts):
        steps = jax.random.uniform(jax.random.fold_in(jax.random.fold_in(stream_key, 6), dim), (parts,), jnp.float32, least / len(pieces), high / len(pieces))
        return jnp.repeat(jnp.exp(steps), shape[dim] // parts).reshape((-1,) + (1,) * (len(shape) - dim - 1))

    factor_of = one(*pieces[0])
    for cut in pieces[1:]:
        factor_of = factor_of * one(*cut)
    return factor_of


def shared_out(stream_key, own, number, rows, amount, top, bound, skew):
    ranking = jax.random.permutation(stream_key, amount)
    heavy_load, ordinary = shares(amount, rows * top, bound, skew, True), shares(amount, rows * top, bound, skew, False)
    places = jnp.arange(amount)

    def named(sizes, rotation):
        used = int((sizes > 0).sum())
        fixed = max(1, used // 4)
        moved = fixed + (places - fixed + rotation * (used - fixed)) % max(1, amount - fixed)
        return jnp.zeros((amount,), jnp.int32).at[ranking[jnp.where(places < fixed, places, moved)]].set(jnp.asarray(sizes, jnp.int32))

    sizes = jnp.where(number % 4 == 0, named(heavy_load, number // 4), named(ordinary, number - number // 4 - 1))
    mixed = jax.random.permutation(jax.random.fold_in(own, 3), amount)
    donor, taker = mixed[0:amount // 2 * 2:2], mixed[1:amount // 2 * 2:2]
    slack = jnp.minimum(sizes[donor] - 1, bound - sizes[taker]) // 2
    slack = jnp.where((donor == ranking[0]) | (taker == ranking[0]) | (sizes[taker] == 0), 0, jnp.maximum(slack, 0))
    moved = jax.random.randint(jax.random.fold_in(own, 4), (amount // 2,), 0, 1 << 20) % (slack + 1)
    sizes = sizes.at[donor].add(-moved).at[taker].add(moved)
    items = jnp.searchsorted(jnp.cumsum(sizes), jnp.arange(rows * top), side="right").astype(jnp.int32)
    table = items.reshape(top, rows).T
    table = table[jax.random.permutation(jax.random.fold_in(own, 1), rows)]
    rotation = jax.random.randint(jax.random.fold_in(own, 2), (rows, 1), 0, top)
    return jnp.take_along_axis(table, (jnp.arange(top)[None, :] + rotation) % top, axis=1)


def shares(number_of, total, reach, lean, full):
    portions = [(1 << 20) // math.isqrt(standing ** lean) + 1 for standing in range(1, number_of + 1)]
    largest = reach if full else min(reach, max(-(-total // number_of), total * portions[0] // sum(portions)))
    least = 1 if total - largest >= number_of - 1 else 0
    given, surplus = [largest] + [least] * (number_of - 1), total - largest - least * (number_of - 1)
    while surplus > 0:
        free = [i for i in range(1, number_of) if given[i] < largest] or [i for i in range(1, number_of) if given[i] < reach]
        mass, budget = sum([portions[i] for i in free]), surplus
        for i in free:
            more = min(reach - given[i], max(1, budget * portions[i] // mass), surplus)
            given[i] = given[i] + more
            surplus = surplus - more
    return np.array(given)


def gaussian(key, shape, deviation, bound, pieces=(), kind=jnp.bfloat16):
    values = deviation * jax.random.normal(key, shape, jnp.float32)
    if pieces:
        values = values * shard_levels(key, shape, pieces, -0.22, 0.18)
    return jnp.clip(values, -bound, bound).astype(kind)


def setup_inputs(seed: int = 0) -> dict:
    seeds = jax.random.split(jax.random.key(seed), 8)
    tokens = draw_tokens(jax.random.fold_in(seeds[7], 71), 0)
    out_grad = gaussian(seeds[1], (TOKENS, D), 0.3, 4.0, ((0, 64),))
    expert_ids_keys = jax.random.split(jax.random.fold_in(seeds[2], 1), TOKENS // TOK_DEV)
    expert_ids_turns = jax.random.permutation(jax.random.fold_in(seeds[2], 3), TOKENS // TOK_DEV)
    expert_ids = jax.vmap(lambda own, number: shared_out(jax.random.fold_in(seeds[2], 2), own, number, TOK_DEV, EXPERTS, TOPK, CAP, 1))(expert_ids_keys, expert_ids_turns).reshape((TOKENS, TOPK))
    router_weight = gaussian(seeds[3], (D, EXPERTS), D ** -0.5, 0.125)
    w_gate = gaussian(seeds[4], (EXPERTS, D, FF), D ** -0.5, 0.125, ((0, 64), (2, 4)))
    w_up = gaussian(seeds[5], (EXPERTS, D, FF), D ** -0.5, 0.125, ((0, 64), (2, 4)))
    w_down = gaussian(seeds[6], (EXPERTS, FF, D), FF ** -0.5, 0.15625, ((0, 64), (1, 4)))
    return {"tokens": tokens, "out_grad": out_grad, "expert_ids": expert_ids, "router_weight": router_weight, "w_gate": w_gate, "w_up": w_up, "w_down": w_down}


def activation_parts(gate_pre, up_pre):
    glu = jnp.minimum(gate_pre, 7.0)
    linear = jnp.clip(up_pre, -7.0, 7.0)
    sigma = jax.nn.sigmoid(1.702 * glu)
    act_value = glu * sigma
    hidden = (linear + 1.0) * act_value
    slope = (linear + 1.0) * (sigma + 1.702 * glu * sigma * (1.0 - sigma))
    slope = jnp.where(gate_pre < 7.0, slope, 0.0)
    up_slope = jnp.where((up_pre > -7.0) & (up_pre < 7.0), act_value, 0.0)
    return hidden, slope, up_slope


def reference(tokens, out_grad, expert_ids, router_weight, w_gate, w_up, w_down):
    logits = jnp.dot(tokens, router_weight, preferred_element_type=jnp.float32)
    chosen = jnp.take_along_axis(logits, expert_ids, axis=1)
    gate_values = jax.nn.softmax(chosen, axis=-1)
    assign_total = TOKENS * TOPK
    slot_total = N_EP * CAP
    flat_ids = expert_ids.reshape(-1)
    flat_tok = (jnp.arange(assign_total, dtype=jnp.int32) // TOPK).astype(jnp.int32)
    flat_gate = gate_values.reshape(-1)

    def per_expert(carry, inputs):
        token_acc, score_acc = carry
        gate_mat, up_mat, down_mat, expert = inputs
        picked = jnp.nonzero(flat_ids == expert, size=slot_total, fill_value=assign_total)[0].astype(jnp.int32)
        valid = picked < assign_total
        safe_pick = jnp.minimum(picked, assign_total - 1).astype(jnp.int32)
        tok_rows = flat_tok[safe_pick]
        inputs_rows = tokens[tok_rows]
        grad_rows = out_grad[tok_rows]
        weight_rows = jnp.where(valid, flat_gate[safe_pick], 0.0)
        gate_pre = jnp.dot(inputs_rows, gate_mat, preferred_element_type=jnp.float32)
        up_pre = jnp.dot(inputs_rows, up_mat, preferred_element_type=jnp.float32)
        hidden, slope, up_slope = activation_parts(gate_pre, up_pre)
        back_proj = jnp.dot(grad_rows, down_mat.T, preferred_element_type=jnp.float32)
        gate_score = jnp.sum(hidden * back_proj, axis=1)
        d_hidden = weight_rows[:, None] * back_proj
        d_gate_pre = (d_hidden * slope).astype(jnp.bfloat16)
        d_up_pre = (d_hidden * up_slope).astype(jnp.bfloat16)
        weighted = (weight_rows[:, None] * hidden).astype(jnp.bfloat16)
        down_grad = jnp.dot(weighted.T, grad_rows, preferred_element_type=jnp.float32).astype(jnp.bfloat16)
        gate_grad = jnp.dot(inputs_rows.T, d_gate_pre, preferred_element_type=jnp.float32).astype(jnp.bfloat16)
        up_grad = jnp.dot(inputs_rows.T, d_up_pre, preferred_element_type=jnp.float32).astype(jnp.bfloat16)
        token_part = jnp.dot(d_gate_pre, gate_mat.T, preferred_element_type=jnp.float32)
        token_part = token_part + jnp.dot(d_up_pre, up_mat.T, preferred_element_type=jnp.float32)
        token_acc = token_acc.at[tok_rows].add(jnp.where(valid[:, None], token_part, 0.0))
        score_acc = score_acc.at[safe_pick].add(jnp.where(valid, gate_score, 0.0))
        return (token_acc, score_acc), (gate_grad, up_grad, down_grad)

    start_carry = (jnp.zeros((TOKENS, D), jnp.float32), jnp.zeros((assign_total,), jnp.float32))
    expert_list = jnp.arange(EXPERTS, dtype=jnp.int32)
    (token_acc, score_acc), (w_gate_grad, w_up_grad, w_down_grad) = lax.scan(
        per_expert, start_carry, (w_gate, w_up, w_down, expert_list))
    gate_score = score_acc.reshape(TOKENS, TOPK)
    d_chosen = gate_values * (gate_score - jnp.sum(gate_values * gate_score, axis=-1, keepdims=True))
    one_hot = (expert_ids[:, :, None] == jnp.arange(EXPERTS, dtype=jnp.int32)[None, None, :]).astype(jnp.float32)
    d_logits = jnp.sum(d_chosen[:, :, None] * one_hot, axis=1)
    router_grad = jnp.dot(tokens.astype(jnp.float32).T, d_logits, precision=lax.Precision.HIGHEST)
    router_part = jnp.dot(d_logits, router_weight.astype(jnp.float32).T, precision=lax.Precision.HIGHEST)
    token_grad = (token_acc + router_part).astype(jnp.bfloat16)
    return token_grad, router_grad, w_gate_grad, w_up_grad, w_down_grad
```

```python
import functools

import jax
import jax.numpy as jnp
from jax import lax
from jax.experimental import pallas as pl
from jax.experimental.pallas import tpu as pltpu
from jax.sharding import PartitionSpec as P

F32 = jnp.float32
BF16 = jnp.bfloat16
HI = lax.Precision.HIGHEST
VMEM = pl.BlockSpec(memory_space=pltpu.VMEM)
SMEM = pl.BlockSpec(memory_space=pltpu.SMEM)


def mm(a, b, dims, precision=None):
    return lax.dot_general(a, b, (dims, ((), ())), precision=precision, preferred_element_type=F32)


NN = ((1,), (0,))
NT = ((1,), (1,))
TN = ((0,), (0,))


def iota(shape, dim):
    return lax.broadcasted_iota(jnp.int32, shape, dim)


def spread(experts, cap):
    rows = experts * cap
    return (iota((rows, experts), 0) // cap == iota((rows, experts), 1)).astype(F32)


def dispatch_kernel(cap, tp_ref, tok_ref, og_ref, ids_ref, rw_ref, send_ref, code_ref, gate_ref):
    n_tok, width = tok_ref.shape
    experts = rw_ref.shape[1]
    share = send_ref.shape[1] // 2
    start = pl.multiple_of(tp_ref[0] * share, share)
    logits = mm(tok_ref[...], rw_ref[...], NN)
    ids = ids_ref[...]
    lane = iota((n_tok, experts), 1)
    hit = lane == ids[:, 0:1]
    for k in range(1, ids.shape[1]):
        hit = hit | (lane == ids[:, k : k + 1])
    mask = hit.astype(F32)
    top = jnp.max(jnp.where(hit, logits, -jnp.inf), axis=1, keepdims=True)
    weight = jnp.where(hit, jnp.exp(jnp.where(hit, logits - top, 0.0)), 0.0)
    gate = weight / jnp.sum(weight, axis=1, keepdims=True)
    earlier = (iota((n_tok, n_tok), 1) < iota((n_tok, n_tok), 0)).astype(BF16)
    rank = mm(earlier, mask.astype(BF16), NN)
    code = mask * (rank + 1.0)
    code_ref[...] = code
    gate_ref[...] = gate
    expand = spread(experts, cap)
    rows = experts * cap
    code_of = mm(expand.astype(BF16), code.astype(BF16), NT)
    pick = code_of == (iota((rows, n_tok), 0) % cap + 1).astype(F32)
    gate_of = jnp.where(pick, mm(expand, gate, NT, HI), 0.0)
    send_ref[:, :share] = mm(pick.astype(F32).astype(BF16), tok_ref[:, pl.ds(start, share)], NN).astype(BF16)
    cot = og_ref[:, pl.ds(start, share)].astype(F32)
    send_ref[:, share:] = mm(gate_of, cot, NN, HI).astype(BF16)


def expert_kernel(cap, tp_ref, own_ref, prev_ref, next_ref, far0_ref, far1_ref, wg_ref, wu_ref, wd_ref,
                  hid_ref, dg_ref, du_ref, score_ref):
    share = own_ref.shape[1] // 2
    rows = own_ref.shape[0]
    half = rows // 2
    me = tp_ref[0]

    def terms(x, at, off):
        start = pl.multiple_of(lax.rem(me + off, 4) * share, share)
        wg = wg_ref[pl.ds(start, share), :]
        wu = wu_ref[pl.ds(start, share), :]
        wd = wd_ref[:, pl.ds(start, share)]
        t = x[at, :share]
        return (mm(t, wg, NN), mm(t, wu, NN), mm(x[at, share:], wd, NT))

    for h in range(2):
        at = pl.ds(h * half, half)
        far = far0_ref if h == 0 else far1_ref
        parts = [terms(own_ref, at, 0), terms(prev_ref, at, 3), terms(next_ref, at, 1),
                 terms(far, pl.ds(0, half), 2)]
        gate_pre = sum(p[0] for p in parts)
        up_pre = sum(p[1] for p in parts)
        back = sum(p[2] for p in parts)
        glu = jnp.minimum(gate_pre, 7.0)
        linear = jnp.clip(up_pre, -7.0, 7.0)
        sig = jax.nn.sigmoid(1.702 * glu)
        act = glu * sig
        hidden = (linear + 1.0) * act
        slope = (linear + 1.0) * (sig + 1.702 * glu * sig * (1.0 - sig))
        slope = jnp.where(gate_pre < 7.0, slope, 0.0)
        up_slope = jnp.where((up_pre > -7.0) & (up_pre < 7.0), act, 0.0)
        hid_ref[at, :] = hidden.astype(BF16)
        dg_ref[at, :] = (back * slope).astype(BF16)
        du_ref[at, :] = (back * up_slope).astype(BF16)
        score = jnp.sum(hidden * back, axis=1, keepdims=True)
        peers = half // cap
        spot = (iota((half, 128), 0) % cap == iota((half, 128), 1)).astype(F32) * score
        group = (iota((peers, half), 1) // cap == iota((peers, half), 0)).astype(F32)
        score_ref[h * peers : (h + 1) * peers, :] = mm(group, spot, NN, HI)


def token_kernel(tp_ref, dg_ref, du_ref, wg_ref, wu_ref, b0_ref, b1_ref, b2_ref, b3_ref):
    share = b0_ref.shape[1]
    me = tp_ref[0]
    dg, du = dg_ref[...], du_ref[...]
    for off, out in ((2, b2_ref), (1, b1_ref), (3, b3_ref), (0, b0_ref)):
        start = pl.multiple_of(lax.rem(me + off, 4) * share, share)
        part = mm(dg, wg_ref[pl.ds(start, share), :], NT) + mm(du, wu_ref[pl.ds(start, share), :], NT)
        out[...] = part.astype(out.dtype)


def weight_kernel(tp_ref, own_ref, prev_ref, next_ref, far0_ref, far1_ref, hid_ref, dg_ref, du_ref,
                  gwg_ref, gwu_ref, gwd_ref):
    share = own_ref.shape[1] // 2
    half = own_ref.shape[0] // 2
    me = tp_ref[0]
    dg, du, hid = dg_ref[...], du_ref[...], hid_ref[...]
    for off, x in ((0, own_ref), (3, prev_ref), (1, next_ref), (2, None)):
        start = pl.multiple_of(lax.rem(me + off, 4) * share, share)
        if x is None:
            t = jnp.concatenate([far0_ref[:, :share], far1_ref[:, :share]], axis=0)
            g = jnp.concatenate([far0_ref[:, share:], far1_ref[:, share:]], axis=0)
        else:
            t = x[:, :share]
            g = x[:, share:]
        gwg_ref[pl.ds(start, share), :] = mm(t, dg, TN).astype(BF16)
        gwu_ref[pl.ds(start, share), :] = mm(t, du, TN).astype(BF16)
        gwd_ref[:, pl.ds(start, share)] = mm(hid, g, TN).astype(BF16)


def router_kernel(cap, tp_ref, q_ref, code_ref, gate_ref, tok_ref, rw_ref, part_ref, term_ref):
    share = part_ref.shape[1]
    start = pl.multiple_of(tp_ref[0] * share, share)
    code, gate = code_ref[...], gate_ref[...]
    q = q_ref[...].T
    score = jnp.zeros_like(code)
    for r in range(cap):
        score = score + jnp.where(code == r + 1.0, q[r : r + 1, :], 0.0)
    d_logits = score - gate * jnp.sum(score, axis=1, keepdims=True)
    part_ref[...] = mm(d_logits, rw_ref[pl.ds(start, share), :].astype(F32), NT, HI)
    term = mm(d_logits, tok_ref[:, pl.ds(start, share)].astype(F32), TN, HI)
    high = term.astype(BF16)
    low = (term - high.astype(F32)).astype(BF16)
    pieces = share // 128
    for j in range(pieces):
        term_ref[:, j, :] = high[:, j * 128 : (j + 1) * 128]
        term_ref[:, pieces + j, :] = low[:, j * 128 : (j + 1) * 128]


def home_kernel(cap, home_ref, code_ref, part_ref, tok_out_ref, router_ref):
    share = part_ref.shape[1]
    code = code_ref[...]
    n_tok, experts = code.shape
    rows = experts * cap
    code_of = mm(code.astype(BF16), spread(experts, cap).astype(BF16), NT)
    pick = code_of == (iota((n_tok, rows), 1) % cap + 1).astype(F32)
    flat = home_ref[...].reshape(rows, home_ref.shape[2])
    tok_out_ref[...] = (
        mm(pick.astype(F32).astype(BF16), flat[:, :share], NN) + part_ref[...]
    ).astype(BF16)
    both = jnp.sum(home_ref[:, :, share:].astype(F32), axis=0)
    pieces = share // 128
    router_ref[...] = both[:pieces] + both[pieces:]


def call(body, outs, n_in, scalar=True):
    return pl.pallas_call(
        body,
        out_shape=outs,
        in_specs=([SMEM] if scalar else []) + [VMEM] * n_in,
        out_specs=[VMEM] * len(outs),
    )


def shape(dims, dtype):
    return jax.ShapeDtypeStruct(dims, dtype)


def per_device(tokens, out_grad, expert_ids, router_weight, w_gate, w_up, w_down):
    n_tok, width = tokens.shape
    experts = router_weight.shape[1]
    peers = lax.axis_size("ep")
    tp = lax.axis_size("tp")
    cap = 8
    share = width // tp
    ff = w_gate.shape[2]
    rows = peers * cap
    half = rows // 2
    me = jnp.full((1,), lax.axis_index("tp"), jnp.int32)

    def hop(value, by):
        return lax.ppermute(value, "tp", [(i, (i + by) % tp) for i in range(tp)])

    def exchange(value):
        return lax.all_to_all(value, "ep", split_axis=0, concat_axis=0, tiled=True)

    send, code, gate = call(
        functools.partial(dispatch_kernel, cap),
        [shape((rows, 2 * share), BF16), shape((n_tok, experts), F32), shape((n_tok, experts), F32)],
        4,
    )(me, tokens, out_grad, expert_ids, router_weight)
    own = exchange(send.reshape(peers, cap, 2 * share)).reshape(rows, 2 * share)
    prev, nxt = hop(own, 1), hop(own, -1)
    far0, far1 = hop(prev[:half], 1), hop(nxt[half:], -1)
    wg, wu, wd = w_gate[0], w_up[0], w_down[0]
    hid, dg, du, score = call(
        functools.partial(expert_kernel, cap),
        [shape((rows, ff), BF16)] * 3 + [shape((peers, 128), F32)],
        8,
    )(me, own, prev, nxt, far0, far1, wg, wu, wd)
    b0, b1, b2, b3 = call(
        token_kernel,
        [shape((rows, share), F32), shape((rows, share), F32), shape((rows, share), BF16),
         shape((rows, share), F32)],
        4,
    )(me, dg, du, wg, wu)
    score = score + hop(score, 1) + hop(score, -1) + hop(score, 2)
    s1, s2 = hop(b2[:half], 1), hop(b2[half:], -1)
    up = jnp.concatenate([b1[:half] + s1.astype(F32), b1[half:]], axis=0).astype(BF16)
    down = jnp.concatenate([b3[:half], b3[half:] + s2.astype(F32)], axis=0).astype(BF16)
    r1, r2 = hop(up, 1), hop(down, -1)
    summed = (b0 + r1.astype(F32) + r2.astype(F32)).astype(BF16)
    gwg, gwu, gwd = call(
        weight_kernel,
        [shape((width, ff), BF16), shape((width, ff), BF16), shape((ff, width), BF16)],
        8,
    )(me, own, prev, nxt, far0, far1, hid, dg, du)
    q = exchange(score.reshape(peers, 1, 128)).reshape(peers, 128)
    part, term = call(
        functools.partial(router_kernel, cap),
        [shape((n_tok, share), F32), shape((peers, cap, 128), BF16)],
        5,
    )(me, q, code, gate, tokens, router_weight)
    payload = jnp.concatenate([summed.reshape(peers, cap, share), term], axis=2)
    home = exchange(payload)
    token_grad, router = call(
        functools.partial(home_kernel, cap),
        [shape((n_tok, share), BF16), shape((share // 128, 128), F32)],
        3,
        scalar=False,
    )(home, code, part)
    return (token_grad, router.reshape(share, 1), gwg[None], gwu[None], gwd[None])


def solution(mesh):
    in_specs = (
        P("ep", None),
        P("ep", None),
        P("ep", None),
        P(),
        P("ep", None, "tp"),
        P("ep", None, "tp"),
        P("ep", "tp", None),
    )
    out_specs = (
        P("ep", "tp"),
        P("tp", "ep"),
        P("ep", None, "tp"),
        P("ep", None, "tp"),
        P("ep", "tp", None),
    )
    return jax.shard_map(
        per_device, mesh=mesh, in_specs=in_specs, out_specs=out_specs, check_vma=False
    )
```

```python
import functools

import jax
import jax.numpy as jnp
from jax import lax
from jax.experimental import pallas as pl
from jax.experimental.pallas import tpu as pltpu
from jax.sharding import PartitionSpec as P

F32 = jnp.float32
BF16 = jnp.bfloat16
HI = lax.Precision.HIGHEST
VMEM = pl.BlockSpec(memory_space=pltpu.VMEM)
SMEM = pl.BlockSpec(memory_space=pltpu.SMEM)


def mm(a, b, dims, precision=None):
    return lax.dot_general(a, b, (dims, ((), ())), precision=precision, preferred_element_type=F32)


NN = ((1,), (0,))
NT = ((1,), (1,))
TN = ((0,), (0,))


def iota(shape, dim):
    return lax.broadcasted_iota(jnp.int32, shape, dim)


def spread(experts, cap):
    rows = experts * cap
    return (iota((rows, experts), 0) // cap == iota((rows, experts), 1)).astype(F32)


def dispatch_kernel(cap, tp_ref, tok_ref, og_ref, ids_ref, rw_ref, send_ref, code_ref, gate_ref):
    n_tok = tok_ref.shape[0]
    experts = rw_ref.shape[0]
    share = send_ref.shape[1] // 2
    start = pl.multiple_of(tp_ref[0] * share, share)
    logits = mm(tok_ref[...], rw_ref[...], NT)
    ids = ids_ref[...].astype(F32).T
    lane = iota((n_tok, experts), 1).astype(F32)
    hit = lane == ids[:, 0:1]
    for k in range(1, ids.shape[1]):
        hit = hit | (lane == ids[:, k : k + 1])
    mask = hit.astype(F32)
    top = jnp.max(jnp.where(hit, logits, -jnp.inf), axis=1, keepdims=True)
    weight = jnp.where(hit, jnp.exp(jnp.where(hit, logits - top, 0.0)), 0.0)
    gate = weight / jnp.sum(weight, axis=1, keepdims=True)
    earlier = (iota((n_tok, n_tok), 1) < iota((n_tok, n_tok), 0)).astype(BF16)
    rank = mm(earlier, mask.astype(BF16), NN)
    code = mask * (rank + 1.0)
    code_ref[...] = code
    gate_ref[...] = gate
    expand = spread(experts, cap)
    rows = experts * cap
    code_of = mm(expand.astype(BF16), code.astype(BF16), NT)
    pick = code_of == (iota((rows, n_tok), 0) % cap + 1).astype(F32)
    gate_of = jnp.where(pick, mm(expand, gate, NT, HI), 0.0)
    send_ref[:, :share] = mm(pick.astype(F32).astype(BF16), tok_ref[:, pl.ds(start, share)], NN).astype(BF16)
    cot = og_ref[:, pl.ds(start, share)].astype(F32)
    send_ref[:, share:] = mm(gate_of, cot, NN, HI).astype(BF16)


def near_kernel(tp_ref, own_ref, p0_ref, p1_ref, n0_ref, n1_ref, wg_ref, wu_ref, wd_ref, gp_ref, up_ref, bk_ref):
    share = own_ref.shape[1] // 2
    half = own_ref.shape[0] // 2
    me = tp_ref[0]
    for h in range(2):
        at = pl.ds(h * half, half)
        blocks = ((0, own_ref[at, :]), (3, (p0_ref, p1_ref)[h][...]), (1, (n0_ref, n1_ref)[h][...]))
        gp, up, bk = [], [], []
        for off, x in blocks:
            start = pl.multiple_of(lax.rem(me + off, 4) * share, share)
            gp.append(mm(x[:, :share], wg_ref[pl.ds(start, share), :], NN))
            up.append(mm(x[:, :share], wu_ref[pl.ds(start, share), :], NN))
            bk.append(mm(x[:, share:], wd_ref[:, pl.ds(start, share)], NT))
        gp_ref[at, :] = sum(gp)
        up_ref[at, :] = sum(up)
        bk_ref[at, :] = sum(bk)


def far_kernel(cap, tp_ref, far0_ref, far1_ref, wg_ref, wu_ref, wd_ref, gp_ref, up_ref, bk_ref,
               hid_ref, dg_ref, du_ref, score_ref, b2a_ref, b2b_ref):
    del tp_ref
    share = far0_ref.shape[1] // 2
    half = far0_ref.shape[0]
    for h in range(2):
        at = pl.ds(h * half, half)
        far = (far0_ref, far1_ref)[h]
        t = far[:, :share]
        gate_pre = gp_ref[at, :] + mm(t, wg_ref[...], NN)
        up_pre = up_ref[at, :] + mm(t, wu_ref[...], NN)
        back = bk_ref[at, :] + mm(far[:, share:], wd_ref[...], NT)
        glu = jnp.minimum(gate_pre, 7.0)
        linear = jnp.clip(up_pre, -7.0, 7.0)
        sig = jax.nn.sigmoid(1.702 * glu)
        act = glu * sig
        hidden = (linear + 1.0) * act
        slope = (linear + 1.0) * (sig + 1.702 * glu * sig * (1.0 - sig))
        slope = jnp.where(gate_pre < 7.0, slope, 0.0)
        up_slope = jnp.where((up_pre > -7.0) & (up_pre < 7.0), act, 0.0)
        dg = (back * slope).astype(BF16)
        du = (back * up_slope).astype(BF16)
        hid_ref[at, :] = hidden.astype(BF16)
        dg_ref[at, :] = dg
        du_ref[at, :] = du
        score = jnp.sum(hidden * back, axis=1, keepdims=True)
        peers = half // cap
        spot = (iota((half, 128), 0) % cap == iota((half, 128), 1)).astype(F32) * score
        group = (iota((peers, half), 1) // cap == iota((peers, half), 0)).astype(F32)
        score_ref[h * peers : (h + 1) * peers, :] = mm(group, spot, NN, HI)
        out = (b2a_ref, b2b_ref)[h]
        out[...] = (mm(dg, wg_ref[...], NT) + mm(du, wu_ref[...], NT)).astype(BF16)


def token_kernel(tp_ref, dg_ref, du_ref, wg_ref, wu_ref, b0_ref, b1a_ref, b1b_ref, b3a_ref, b3b_ref):
    share = b0_ref.shape[1]
    half = b0_ref.shape[0] // 2
    me = tp_ref[0]
    for off, lo, hi in ((1, b1a_ref, b1b_ref), (3, b3a_ref, b3b_ref), (0, b0_ref.at[:half], b0_ref.at[half:])):
        start = pl.multiple_of(lax.rem(me + off, 4) * share, share)
        wg, wu = wg_ref[pl.ds(start, share), :], wu_ref[pl.ds(start, share), :]
        for h, out in ((0, lo), (1, hi)):
            at = pl.ds(h * half, half)
            out[...] = (mm(dg_ref[at, :], wg, NT) + mm(du_ref[at, :], wu, NT)).astype(out.dtype)


def weight_kernel(tp_ref, own_ref, p0_ref, p1_ref, n0_ref, n1_ref, far0_ref, far1_ref, hid_ref, dg_ref, du_ref,
                  gwg_ref, gwu_ref, gwd_ref):
    share = own_ref.shape[1] // 2
    half = own_ref.shape[0] // 2
    me = tp_ref[0]
    dg, du, hid = dg_ref[...], du_ref[...], hid_ref[...]
    for off, lo, hi in ((0, own_ref.at[:half], own_ref.at[half:]), (3, p0_ref, p1_ref), (1, n0_ref, n1_ref),
                        (2, far0_ref, far1_ref)):
        start = pl.multiple_of(lax.rem(me + off, 4) * share, share)
        t = jnp.concatenate([lo[:, :share], hi[:, :share]], axis=0)
        g = jnp.concatenate([lo[:, share:], hi[:, share:]], axis=0)
        gwg_ref[pl.ds(start, share), :] = mm(t, dg, TN).astype(BF16)
        gwu_ref[pl.ds(start, share), :] = mm(t, du, TN).astype(BF16)
        gwd_ref[:, pl.ds(start, share)] = mm(hid, g, TN).astype(BF16)


def router_kernel(cap, tp_ref, q_ref, code_ref, gate_ref, tok_ref, rw_ref, part_ref, term_ref):
    share = part_ref.shape[1]
    start = pl.multiple_of(tp_ref[0] * share, share)
    code, gate = code_ref[...], gate_ref[...]
    q = q_ref[...].T
    score = jnp.zeros_like(code)
    for r in range(cap):
        score = score + jnp.where(code == r + 1.0, q[r : r + 1, :], 0.0)
    d_logits = score - gate * jnp.sum(score, axis=1, keepdims=True)
    part_ref[...] = mm(d_logits, rw_ref[:, pl.ds(start, share)].astype(F32), NN, HI)
    term = mm(d_logits, tok_ref[:, pl.ds(start, share)].astype(F32), TN, HI)
    high = term.astype(BF16)
    low = (term - high.astype(F32)).astype(BF16)
    pieces = share // 128
    for j in range(pieces):
        term_ref[:, j, :] = high[:, j * 128 : (j + 1) * 128]
        term_ref[:, pieces + j, :] = low[:, j * 128 : (j + 1) * 128]


def home_kernel(cap, home_ref, code_ref, part_ref, tok_out_ref, router_ref):
    share = part_ref.shape[1]
    code = code_ref[...]
    n_tok, experts = code.shape
    rows = experts * cap
    code_of = mm(code.astype(BF16), spread(experts, cap).astype(BF16), NT)
    pick = code_of == (iota((n_tok, rows), 1) % cap + 1).astype(F32)
    flat = home_ref[...].reshape(rows, home_ref.shape[2])
    tok_out_ref[...] = (
        mm(pick.astype(F32).astype(BF16), flat[:, :share], NN) + part_ref[...]
    ).astype(BF16)
    both = jnp.sum(home_ref[:, :, share:].astype(F32), axis=0)
    pieces = share // 128
    router_ref[...] = both[:pieces] + both[pieces:]


def cost(flops, data):
    return pl.CostEstimate(flops=flops, bytes_accessed=data, transcendentals=0)


def call(body, outs, n_in, flops, scalar=True):
    return pl.pallas_call(
        body,
        out_shape=outs,
        in_specs=([SMEM] if scalar else []) + [VMEM] * n_in,
        out_specs=[VMEM] * len(outs),
        cost_estimate=cost(flops, 4 << 20),
    )


def shape(dims, dtype):
    return jax.ShapeDtypeStruct(dims, dtype)


def per_device(tokens, out_grad, expert_ids, router_weight, w_gate, w_up, w_down):
    n_tok, width = tokens.shape
    experts = router_weight.shape[1]
    peers = lax.axis_size("ep")
    tp = lax.axis_size("tp")
    cap = 8
    share = width // tp
    ff = w_gate.shape[2]
    rows = peers * cap
    half = rows // 2
    me = jnp.full((1,), lax.axis_index("tp"), jnp.int32)
    unit = 2 * rows * share * ff
    router_t = router_weight.T

    def hop(value, by):
        return lax.ppermute(value, "tp", [(i, (i + by) % tp) for i in range(tp)])

    def exchange(value):
        return lax.all_to_all(value, "ep", split_axis=0, concat_axis=0, tiled=True)

    send, code, gate = call(
        functools.partial(dispatch_kernel, cap),
        [shape((rows, 2 * share), BF16), shape((n_tok, experts), F32), shape((n_tok, experts), F32)],
        4,
        unit,
    )(me, tokens, out_grad, expert_ids.T, router_t)
    own = exchange(send.reshape(peers, cap, 2 * share)).reshape(rows, 2 * share)
    p0, n1 = hop(own[:half], 1), hop(own[half:], -1)
    p1, n0 = hop(own[half:], 1), hop(own[:half], -1)
    far0, far1 = hop(p0, 1), hop(n1, -1)
    wg, wu, wd = w_gate[0], w_up[0], w_down[0]
    near = call(near_kernel, [shape((rows, ff), F32)] * 3, 8, 9 * unit)(me, own, p0, p1, n0, n1, wg, wu, wd)

    def far_block(i, tp_ref):
        return (lax.rem(tp_ref[0] + 2, 4), 0)

    def far_column(i, tp_ref):
        return (0, lax.rem(tp_ref[0] + 2, 4))

    def whole(dims):
        return pl.BlockSpec(dims, lambda i, tp_ref: (0, 0))

    far_outs = [shape((rows, ff), BF16)] * 3 + [shape((peers, 128), F32)] + [shape((half, share), BF16)] * 2
    hid, dg, du, score, b2a, b2b = pl.pallas_call(
        functools.partial(far_kernel, cap),
        out_shape=far_outs,
        grid_spec=pltpu.PrefetchScalarGridSpec(
            num_scalar_prefetch=1,
            grid=(1,),
            in_specs=[
                whole((half, 2 * share)),
                whole((half, 2 * share)),
                pl.BlockSpec((share, ff), far_block),
                pl.BlockSpec((share, ff), far_block),
                pl.BlockSpec((ff, share), far_column),
            ]
            + [whole((rows, ff))] * 3,
            out_specs=[whole(o.shape) for o in far_outs],
        ),
        cost_estimate=cost(5 * unit, 4 << 20),
    )(me, far0, far1, wg, wu, wd, *near)
    score = score + hop(score, 1) + hop(score, -1) + hop(score, 2)
    s1, s2 = hop(b2a, 1), hop(b2b, -1)
    b0, b1a, b1b, b3a, b3b = call(
        token_kernel,
        [shape((rows, share), F32), shape((half, share), F32), shape((half, share), BF16),
         shape((half, share), BF16), shape((half, share), F32)],
        4,
        6 * unit,
    )(me, dg, du, wg, wu)
    d1, d2 = hop(b1b, 1), hop(b3a, -1)
    e1 = hop((b1a + s1.astype(F32)).astype(BF16), 1)
    e2 = hop((b3b + s2.astype(F32)).astype(BF16), -1)
    summed = b0 + jnp.concatenate(
        [e1.astype(F32) + d2.astype(F32), d1.astype(F32) + e2.astype(F32)], axis=0
    )
    gwg, gwu, gwd = call(
        weight_kernel,
        [shape((width, ff), BF16), shape((width, ff), BF16), shape((ff, width), BF16)],
        10,
        12 * unit,
    )(me, own, p0, p1, n0, n1, far0, far1, hid, dg, du)
    q = exchange(score.reshape(peers, 1, 128)).reshape(peers, 128)
    part, term = call(
        functools.partial(router_kernel, cap),
        [shape((n_tok, share), F32), shape((peers, cap, 128), BF16)],
        5,
        unit,
    )(me, q, code, gate, tokens, router_t)
    payload = jnp.concatenate([summed.astype(BF16).reshape(peers, cap, share), term], axis=2)
    home = exchange(payload)
    token_grad, router = call(
        functools.partial(home_kernel, cap),
        [shape((n_tok, share), BF16), shape((share // 128, 128), F32)],
        3,
        unit,
        scalar=False,
    )(home, code, part)
    return (token_grad, router.reshape(share, 1), gwg[None], gwu[None], gwd[None])


def solution(mesh):
    in_specs = (
        P("ep", None),
        P("ep", None),
        P("ep", None),
        P(),
        P("ep", None, "tp"),
        P("ep", None, "tp"),
        P("ep", "tp", None),
    )
    out_specs = (
        P("ep", "tp"),
        P("tp", "ep"),
        P("ep", None, "tp"),
        P("ep", None, "tp"),
        P("ep", "tp", None),
    )
    return jax.shard_map(
        per_device, mesh=mesh, in_specs=in_specs, out_specs=out_specs, check_vma=False
    )
```

```python
import functools

import jax
import jax.numpy as jnp
from jax import lax
from jax.experimental import pallas as pl
from jax.experimental.pallas import tpu as pltpu
from jax.sharding import PartitionSpec as P


F32 = jnp.float32
BF16 = jnp.bfloat16
HI = lax.Precision.HIGHEST
VMEM = pl.BlockSpec(memory_space=pltpu.VMEM)
SMEM = pl.BlockSpec(memory_space=pltpu.SMEM)


def mm(a, b, dims, precision=None):
    return lax.dot_general(a, b, (dims, ((), ())), precision=precision, preferred_element_type=F32)


NN = ((1,), (0,))
NT = ((1,), (1,))
TN = ((0,), (0,))


def iota(shape, dim):
    return lax.broadcasted_iota(jnp.int32, shape, dim)


def spread(experts, cap):
    rows = experts * cap
    return (iota((rows, experts), 0) // cap == iota((rows, experts), 1)).astype(F32)


def dispatch_kernel(cap, tp_ref, tok_ref, og_ref, ids_ref, rw_ref, send_ref, code_ref, gate_ref):
    n_tok = tok_ref.shape[0]
    experts = rw_ref.shape[0]
    share = send_ref.shape[1] // 2
    start = pl.multiple_of(tp_ref[0] * share, share)
    logits = mm(tok_ref[...], rw_ref[...], NT)
    ids = ids_ref[...].astype(F32).T
    lane = iota((n_tok, experts), 1).astype(F32)
    hit = lane == ids[:, 0:1]
    for k in range(1, ids.shape[1]):
        hit = hit | (lane == ids[:, k : k + 1])
    mask = hit.astype(F32)
    top = jnp.max(jnp.where(hit, logits, -jnp.inf), axis=1, keepdims=True)
    weight = jnp.where(hit, jnp.exp(jnp.where(hit, logits - top, 0.0)), 0.0)
    gate = weight / jnp.sum(weight, axis=1, keepdims=True)
    earlier = (iota((n_tok, n_tok), 1) < iota((n_tok, n_tok), 0)).astype(BF16)
    rank = mm(earlier, mask.astype(BF16), NN)
    code = mask * (rank + 1.0)
    code_ref[...] = code
    gate_ref[...] = gate
    expand = spread(experts, cap)
    rows = experts * cap
    code_of = mm(expand.astype(BF16), code.astype(BF16), NT)
    pick = code_of == (iota((rows, n_tok), 0) % cap + 1).astype(F32)
    gate_of = jnp.where(pick, mm(expand, gate, NT, HI), 0.0)
    send_ref[:, :share] = mm(pick.astype(F32).astype(BF16), tok_ref[:, pl.ds(start, share)], NN).astype(BF16)
    cot = og_ref[:, pl.ds(start, share)].astype(F32)
    send_ref[:, share:] = mm(gate_of, cot, NN, HI).astype(BF16)


def expert_kernel(cap, first, tp_ref, own_ref, p0_ref, p1_ref, n0_ref, n1_ref, f0_ref, f1_ref, wg_ref, wu_ref, wd_ref,
                  hid_ref, dg_ref, du_ref, score_ref, plus_ref, minus_ref, b1_ref, b3_ref, b0_ref):
    rows, share = b0_ref.shape
    half = rows // 2
    me = tp_ref[0]

    def at(off):
        return pl.ds(pl.multiple_of(lax.rem(me + off, 4) * share, share), share)

    def joined(lo, hi, cols):
        return jnp.concatenate([lo[:, cols], hi[:, cols]], axis=0)

    left, right = slice(0, share), slice(share, 2 * share)
    gate_pre = up_pre = back = None
    for off, lo, hi in ((0, own_ref.at[pl.ds(first, half)], own_ref.at[pl.ds(first + half, half)]),
                        (3, p0_ref, p1_ref), (1, n0_ref, n1_ref), (2, f0_ref, f1_ref)):
        t, g = joined(lo, hi, left), joined(lo, hi, right)
        terms = (mm(t, wg_ref[at(off), :], NN), mm(t, wu_ref[at(off), :], NN), mm(g, wd_ref[:, at(off)], NT))
        if gate_pre is None:
            gate_pre, up_pre, back = terms
        else:
            gate_pre, up_pre, back = gate_pre + terms[0], up_pre + terms[1], back + terms[2]
    glu = jnp.minimum(gate_pre, 7.0)
    linear = jnp.clip(up_pre, -7.0, 7.0)
    sig = jax.nn.sigmoid(1.702 * glu)
    act = glu * sig
    hidden = (linear + 1.0) * act
    slope = (linear + 1.0) * (sig + 1.702 * glu * sig * (1.0 - sig))
    slope = jnp.where(gate_pre < 7.0, slope, 0.0)
    up_slope = jnp.where((up_pre > -7.0) & (up_pre < 7.0), act, 0.0)
    dg = (back * slope).astype(BF16)
    du = (back * up_slope).astype(BF16)
    hid_ref[...] = hidden.astype(BF16)
    dg_ref[...] = dg
    du_ref[...] = du
    score = jnp.sum(hidden * back, axis=1, keepdims=True)
    peers = rows // cap
    spot = (iota((rows, 128), 0) % cap == iota((rows, 128), 1)).astype(F32) * score
    group = (iota((peers, rows), 1) // cap == iota((peers, rows), 0)).astype(F32)
    score_ref[...] = mm(group, spot, NN, HI)

    def part(off):
        return mm(dg, wg_ref[at(off), :], NT) + mm(du, wu_ref[at(off), :], NT)

    far = part(2).astype(BF16)
    plus_ref[:half, :] = far[:half]
    minus_ref[half:, :] = far[half:]
    ahead = part(1)
    b1_ref[...] = ahead[:half]
    plus_ref[half:, :] = ahead[half:].astype(BF16)
    behind = part(3)
    minus_ref[:half, :] = behind[:half].astype(BF16)
    b3_ref[...] = behind[half:]
    b0_ref[...] = part(0)


def weight_kernel(tp_ref, own, p0, p1a, p1b, n0, n1a, n1b, f0a, f0b, f1a, f1b, hid0, hid1, dg0, dg1, du0, du1,
                  gwg_ref, gwu_ref, gwd_ref):
    share = own.shape[1] // 2
    me = tp_ref[0]

    def rows(pieces, cols):
        return jnp.concatenate([x[:, cols] for x in pieces], axis=0)

    every = slice(None)
    hid, dg, du = rows((hid0, hid1), every), rows((dg0, dg1), every), rows((du0, du1), every)
    for off, pieces in ((0, (own,)), (3, (p0, p1a, p1b)), (1, (n0, n1b, n1a)), (2, (f0a, f0b, f1a, f1b))):
        at = pl.ds(pl.multiple_of(lax.rem(me + off, 4) * share, share), share)
        t = rows(pieces, slice(0, share))
        g = rows(pieces, slice(share, 2 * share))
        gwg_ref[at, :] = mm(t, dg, TN).astype(BF16)
        gwu_ref[at, :] = mm(t, du, TN).astype(BF16)
        gwd_ref[:, at] = mm(hid, g, TN).astype(BF16)


def router_kernel(cap, tp_ref, q_ref, code_ref, gate_ref, tok_ref, rw_ref, part_ref, term_ref):
    share = part_ref.shape[1]
    start = pl.multiple_of(tp_ref[0] * share, share)
    code, gate = code_ref[...], gate_ref[...]
    q = q_ref[...].T
    score = jnp.zeros_like(code)
    for r in range(cap):
        score = score + jnp.where(code == r + 1.0, q[r : r + 1, :], 0.0)
    d_logits = score - gate * jnp.sum(score, axis=1, keepdims=True)
    part_ref[...] = mm(d_logits, rw_ref[:, pl.ds(start, share)].astype(F32), NN, HI)
    term = mm(d_logits, tok_ref[:, pl.ds(start, share)].astype(F32), TN, HI)
    high = term.astype(BF16)
    low = (term - high.astype(F32)).astype(BF16)
    pieces = share // 128
    for j in range(pieces):
        term_ref[:, j, :] = high[:, j * 128 : (j + 1) * 128]
        term_ref[:, pieces + j, :] = low[:, j * 128 : (j + 1) * 128]


def home_kernel(cap, home_ref, code_ref, part_ref, tok_out_ref, router_ref):
    share = part_ref.shape[1]
    code = code_ref[...]
    n_tok, experts = code.shape
    rows = experts * cap
    code_of = mm(code.astype(BF16), spread(experts, cap).astype(BF16), NT)
    pick = code_of == (iota((n_tok, rows), 1) % cap + 1).astype(F32)
    flat = home_ref[...].reshape(rows, home_ref.shape[2])
    tok_out_ref[...] = (
        mm(pick.astype(F32).astype(BF16), flat[:, :share], NN) + part_ref[...]
    ).astype(BF16)
    both = jnp.sum(home_ref[:, :, share:].astype(F32), axis=0)
    pieces = share // 128
    router_ref[...] = both[:pieces] + both[pieces:]


def cost(flops, data):
    return pl.CostEstimate(flops=flops, bytes_accessed=data, transcendentals=0)


def call(body, outs, n_in, flops, scalar=True):
    return pl.pallas_call(
        body,
        out_shape=outs,
        in_specs=([SMEM] if scalar else []) + [VMEM] * n_in,
        out_specs=[VMEM] * len(outs),
        cost_estimate=cost(flops, 4 << 20),
    )


def shape(dims, dtype):
    return jax.ShapeDtypeStruct(dims, dtype)


def per_device(tokens, out_grad, expert_ids, router_weight, w_gate, w_up, w_down):
    n_tok, width = tokens.shape
    experts = router_weight.shape[1]
    peers = lax.axis_size("ep")
    tp = lax.axis_size("tp")
    cap = 8
    share = width // tp
    ff = w_gate.shape[2]
    rows = peers * cap
    half = rows // 2
    me = jnp.full((1,), lax.axis_index("tp"), jnp.int32)
    unit = 2 * rows * share * ff
    router_t = router_weight.T

    def hop(value, by):
        return lax.ppermute(value, "tp", [(i, (i + by) % tp) for i in range(tp)])

    def exchange(value):
        return lax.all_to_all(value, "ep", split_axis=0, concat_axis=0, tiled=True)

    send, code, gate = call(
        functools.partial(dispatch_kernel, cap),
        [shape((rows, 2 * share), BF16), shape((n_tok, experts), F32), shape((n_tok, experts), F32)],
        4,
        unit,
    )(me, tokens, out_grad, expert_ids.T, router_t)
    own = exchange(send.reshape(peers, cap, 2 * share)).reshape(rows, 2 * share)
    piece = half // 2
    own1a, own1b = own[half : half + piece], own[half + piece :]
    p0, n0 = hop(own[:half], 1), hop(own[:half], -1)
    p1a, n1a = hop(own1a, 1), hop(own1b, -1)
    f0a, f0b = hop(p0[:piece], 1), hop(n0[piece:], -1)
    p1b, n1b = hop(own1b, 1), hop(own1a, -1)
    f1a, f1b = hop(p1a, 1), hop(n1a, -1)
    wg, wu, wd = w_gate[0], w_up[0], w_down[0]

    def expert(h, *blocks):
        hid, dg, du, score, plus, minus, b1, b3, b0 = call(
            functools.partial(expert_kernel, cap, h * half),
            [shape((half, ff), BF16)] * 3
            + [shape((half // cap, 128), F32)]
            + [shape((half, share), BF16)] * 2
            + [shape((piece, share), F32)] * 2
            + [shape((half, share), F32)],
            10,
            10 * unit,
        )(me, own, *blocks, wg, wu, wd)
        rp, rm = hop(plus, 1), hop(minus, -1)
        ep = hop((b1 + rp[:piece].astype(F32)).astype(BF16), 1)
        em = hop((b3 + rm[piece:].astype(F32)).astype(BF16), -1)
        top = b0[:piece] + ep.astype(F32) + rm[:piece].astype(F32)
        low = b0[piece:] + rp[piece:].astype(F32) + em.astype(F32)
        return hid, dg, du, score, [top, low]

    hid0, dg0, du0, score0, sum0 = expert(0, p0[:piece], p0[piece:], n0[:piece], n0[piece:], f0a, f0b)
    hid1, dg1, du1, score1, sum1 = expert(1, p1a, p1b, n1b, n1a, f1a, f1b)
    score = jnp.concatenate([score0, score1], axis=0)
    score = score + hop(score, 1) + hop(score, -1) + hop(score, 2)
    summed = jnp.concatenate(sum0 + sum1, axis=0)
    gwg, gwu, gwd = call(
        weight_kernel,
        [shape((width, ff), BF16), shape((width, ff), BF16), shape((ff, width), BF16)],
        17,
        12 * unit,
    )(me, own, p0, p1a, p1b, n0, n1a, n1b, f0a, f0b, f1a, f1b, hid0, hid1, dg0, dg1, du0, du1)
    q = exchange(score.reshape(peers, 1, 128)).reshape(peers, 128)
    part, term = call(
        functools.partial(router_kernel, cap), [shape((n_tok, share), F32), shape((peers, cap, 128), BF16)], 5, unit
    )(me, q, code, gate, tokens, router_t)
    payload = jnp.concatenate([summed.astype(BF16).reshape(peers, cap, share), term], axis=2)
    home = exchange(payload)
    token_grad, router = call(
        functools.partial(home_kernel, cap),
        [shape((n_tok, share), BF16), shape((share // 128, 128), F32)],
        3,
        unit,
        scalar=False,
    )(home, code, part)
    return (token_grad, router.reshape(share, 1), gwg[None], gwu[None], gwd[None])


def solution(mesh):
    in_specs = (
        P("ep", None),
        P("ep", None),
        P("ep", None),
        P(),
        P("ep", None, "tp"),
        P("ep", None, "tp"),
        P("ep", "tp", None),
    )
    out_specs = (
        P("ep", "tp"),
        P("tp", "ep"),
        P("ep", None, "tp"),
        P("ep", None, "tp"),
        P("ep", "tp", None),
    )

    return jax.shard_map(per_device, mesh=mesh, in_specs=in_specs, out_specs=out_specs, check_vma=False)
```

```python
import functools

import jax
import jax.numpy as jnp
from jax import lax
from jax.experimental import pallas as pl
from jax.experimental.pallas import tpu as pltpu
from jax.sharding import PartitionSpec as P


F32 = jnp.float32
BF16 = jnp.bfloat16
HI = lax.Precision.HIGHEST
VMEM = pl.BlockSpec(memory_space=pltpu.VMEM)
SMEM = pl.BlockSpec(memory_space=pltpu.SMEM)


def mm(a, b, dims, precision=None):
    return lax.dot_general(a, b, (dims, ((), ())), precision=precision, preferred_element_type=F32)


NN = ((1,), (0,))
NT = ((1,), (1,))
TN = ((0,), (0,))


def iota(shape, dim):
    return lax.broadcasted_iota(jnp.int32, shape, dim)


def bits(cap):
    return cap.bit_length() - 1


def spread(experts, cap):
    rows = experts * cap
    return ((iota((rows, experts), 0) >> bits(cap)) == iota((rows, experts), 1)).astype(F32)


def dispatch_kernel(cap, tp_ref, tok_ref, og_ref, ids_ref, rw_ref, send_ref, code_ref, gate_ref):
    n_tok = tok_ref.shape[0]
    experts = rw_ref.shape[0]
    share = send_ref.shape[1] // 2
    start = pl.multiple_of(tp_ref[0] * share, share)
    logits = mm(tok_ref[...], rw_ref[...], NT)
    ids = ids_ref[...].astype(F32).T
    lane = iota((n_tok, experts), 1).astype(F32)
    hit = lane == ids[:, 0:1]
    for k in range(1, ids.shape[1]):
        hit = hit | (lane == ids[:, k : k + 1])
    mask = hit.astype(F32)
    top = jnp.max(jnp.where(hit, logits, -jnp.inf), axis=1, keepdims=True)
    weight = jnp.where(hit, jnp.exp(jnp.where(hit, logits - top, 0.0)), 0.0)
    gate = weight / jnp.sum(weight, axis=1, keepdims=True)
    earlier = (iota((n_tok, n_tok), 1) < iota((n_tok, n_tok), 0)).astype(BF16)
    rank = mm(earlier, mask.astype(BF16), NN)
    code = mask * (rank + 1.0)
    code_ref[...] = code
    gate_ref[...] = gate
    expand = spread(experts, cap)
    rows = experts * cap
    code_of = mm(expand.astype(BF16), code.astype(BF16), NT)
    pick = code_of == ((iota((rows, n_tok), 0) & (cap - 1)) + 1).astype(F32)
    gate_of = jnp.where(pick, mm(expand, gate, NT, HI), 0.0)
    send_ref[:, :share] = mm(pick.astype(F32).astype(BF16), tok_ref[:, pl.ds(start, share)], NN).astype(BF16)
    cot = og_ref[:, pl.ds(start, share)].astype(F32)
    send_ref[:, share:] = mm(gate_of, cot, NN, HI).astype(BF16)


LEFT, RIGHT = 0, 1


def joined(refs, side):
    share = refs[0].shape[1] // 2
    return jnp.concatenate([r[:, side * share : (side + 1) * share] for r in refs], axis=0)


def block(tp_ref, off, share):
    return pl.ds(pl.multiple_of(lax.rem(tp_ref[0] + off, 4) * share, share), share)


def fetch(tp_ref, offs, share, hbm, vmem, sems):
    copies = {}
    for i, off in enumerate(offs):
        at = block(tp_ref, off, share)
        row = []
        for j, (source, target) in enumerate(zip(hbm, vmem)):
            where = (slice(None), at) if j == 2 else (at, slice(None))
            row.append(pltpu.make_async_copy(source.at[where], target.at[where], sems.at[i * len(hbm) + j]))
            row[-1].start()
        copies[off] = row
    return copies


def forward(tp_ref, groups, copies, share, wg, wu, wd, start=None):
    total = start
    for off, refs in groups:
        for copy in copies[off]:
            copy.wait()
        at = block(tp_ref, off, share)
        t, g = joined(refs, LEFT), joined(refs, RIGHT)
        terms = (mm(t, wg[at, :], NN), mm(t, wu[at, :], NN), mm(g, wd[:, at], NT))
        total = terms if total is None else tuple(a + b for a, b in zip(total, terms))
    return total


def units(cap, gate_pre, up_pre, back):
    rows = gate_pre.shape[0]
    glu = jnp.minimum(gate_pre, 7.0)
    linear = jnp.clip(up_pre, -7.0, 7.0)
    sig = jax.nn.sigmoid(1.702 * glu)
    act = glu * sig
    hidden = (linear + 1.0) * act
    slope = (linear + 1.0) * (sig + 1.702 * glu * sig * (1.0 - sig))
    slope = jnp.where(gate_pre < 7.0, slope, 0.0)
    up_slope = jnp.where((up_pre > -7.0) & (up_pre < 7.0), act, 0.0)
    score = jnp.sum(hidden * back, axis=1, keepdims=True)
    peers = rows // cap
    spot = ((iota((rows, 128), 0) & (cap - 1)) == iota((rows, 128), 1)).astype(F32) * score
    group = ((iota((peers, rows), 1) >> bits(cap)) == iota((peers, rows), 0)).astype(F32)
    return (
        hidden.astype(BF16),
        (back * slope).astype(BF16),
        (back * up_slope).astype(BF16),
        mm(group, spot, NN, HI),
    )


def token_parts(tp_ref, dg, du, wg, wu, outs, copies=None):
    plus_ref, minus_ref, b1_ref, b3_ref, b0_ref = outs
    rows, share = b0_ref.shape
    half = rows // 2

    def part(off):
        for copy in copies[off] if copies else ():
            copy.wait()
        at = block(tp_ref, off, share)
        return mm(dg, wg[at, :], NT) + mm(du, wu[at, :], NT)

    far = part(2).astype(BF16)
    plus_ref[:half, :] = far[:half]
    minus_ref[half:, :] = far[half:]
    ahead = part(1)
    b1_ref[...] = ahead[:half]
    plus_ref[half:, :] = ahead[half:].astype(BF16)
    behind = part(3)
    minus_ref[:half, :] = behind[:half].astype(BF16)
    b3_ref[...] = behind[half:]
    b0_ref[...] = part(0)


def first_kernel(cap, tp_ref, own, p0, n0, f0a, f0b, wg_hbm, wu_hbm, wd_hbm,
                 hid_ref, dg_ref, du_ref, score_ref, plus_ref, minus_ref, b1_ref, b3_ref, b0_ref,
                 wg, wu, wd, sems):
    share = b0_ref.shape[1]
    copies = fetch(tp_ref, (0, 3, 1, 2), share, (wg_hbm, wu_hbm, wd_hbm), (wg, wu, wd), sems)
    groups = ((0, (own,)), (3, (p0,)), (1, (n0,)), (2, (f0a, f0b)))
    hid, dg, du, score = units(cap, *forward(tp_ref, groups, copies, share, wg, wu, wd))
    hid_ref[...], dg_ref[...], du_ref[...], score_ref[...] = hid, dg, du, score
    token_parts(tp_ref, dg, du, wg, wu, (plus_ref, minus_ref, b1_ref, b3_ref, b0_ref))


def near_kernel(tp_ref, own, p1a, p1b, n1a, n1b, wg_hbm, wu_hbm, wd_hbm, gp_ref, up_ref, bk_ref, wg, wu, wd, sems):
    share = own.shape[1] // 2
    copies = fetch(tp_ref, (0, 3, 1), share, (wg_hbm, wu_hbm, wd_hbm), (wg, wu, wd), sems)
    groups = ((0, (own,)), (3, (p1a, p1b)), (1, (n1b, n1a)))
    gp_ref[...], up_ref[...], bk_ref[...] = forward(tp_ref, groups, copies, share, wg, wu, wd)


def far_kernel(cap, tp_ref, f1a, f1b, gp, up, bk, score0, wg_hbm, wu_hbm, wd_hbm,
               hid_ref, dg_ref, du_ref, score_ref, wg, wu, wd, sems):
    share = f1a.shape[1] // 2
    copies = fetch(tp_ref, (2,), share, (wg_hbm, wu_hbm, wd_hbm), (wg, wu, wd), sems)
    start = (gp[...], up[...], bk[...])
    hid, dg, du, score = units(cap, *forward(tp_ref, ((2, (f1a, f1b)),), copies, share, wg, wu, wd, start))
    hid_ref[...], dg_ref[...], du_ref[...] = hid, dg, du
    score_ref[...] = jnp.concatenate([score0[...], score], axis=0)


def token_kernel(tp_ref, dg_ref, du_ref, wg_hbm, wu_hbm, plus_ref, minus_ref, b1_ref, b3_ref, b0_ref, wg, wu, sems):
    share = b0_ref.shape[1]
    copies = fetch(tp_ref, (2, 1, 3, 0), share, (wg_hbm, wu_hbm), (wg, wu), sems)
    token_parts(tp_ref, dg_ref[...], du_ref[...], wg, wu, (plus_ref, minus_ref, b1_ref, b3_ref, b0_ref), copies)


def weight_kernel(tp_ref, own, p0, p1a, p1b, n0, n1a, n1b, f0a, f0b, f1a, f1b, hid0, hid1, dg0, dg1, du0, du1,
                  d_logits_ref, rw_ref, gwg_ref, gwu_ref, gwd_ref, part_ref):
    share = own.shape[1] // 2
    part_ref[...] = mm(d_logits_ref[...], rw_ref[:, block(tp_ref, 0, share)].astype(F32), NN, HI)

    def rows(a, b):
        return jnp.concatenate([a[...], b[...]], axis=0)

    hid, dg, du = rows(hid0, hid1), rows(dg0, dg1), rows(du0, du1)
    for off, refs in ((0, (own,)), (3, (p0, p1a, p1b)), (1, (n0, n1b, n1a)), (2, (f0a, f0b, f1a, f1b))):
        at = block(tp_ref, off, share)
        t, g = joined(refs, LEFT), joined(refs, RIGHT)
        gwg_ref[at, :] = mm(t, dg, TN).astype(BF16)
        gwu_ref[at, :] = mm(t, du, TN).astype(BF16)
        gwd_ref[:, at] = mm(hid, g, TN).astype(BF16)


def router_kernel(cap, tp_ref, q_ref, code_ref, gate_ref, tok_ref, *refs):
    sums, (payload_ref, d_logits_ref) = refs[:10], refs[10:]
    share = sums[0].shape[1]
    for h in range(2):
        b0, rp, rm, ep, em = sums[5 * h : 5 * h + 5]
        half = b0.shape[0] // 2
        top = b0[:half] + ep[...].astype(F32) + rm[:half].astype(F32)
        low = b0[half:] + rp[half:].astype(F32) + em[...].astype(F32)
        for i, value in enumerate((top, low)):
            n = half // cap
            at = pl.ds((2 * h + i) * n, n)
            payload_ref[at, :, :share] = value.astype(BF16).reshape(n, cap, share)
    code, gate = code_ref[...], gate_ref[...]
    q = q_ref[...].T
    score = jnp.zeros_like(code)
    for r in range(cap):
        score = score + jnp.where(code == r + 1.0, q[r : r + 1, :], 0.0)
    d_logits = score - gate * jnp.sum(score, axis=1, keepdims=True)
    d_logits_ref[...] = d_logits
    term = mm(d_logits, tok_ref[:, block(tp_ref, 0, share)].astype(F32), TN, HI)
    high = term.astype(BF16)
    low = (term - high.astype(F32)).astype(BF16)
    pieces = share // 128
    for j in range(pieces):
        payload_ref[:, j, share:] = high[:, j * 128 : (j + 1) * 128]
        payload_ref[:, pieces + j, share:] = low[:, j * 128 : (j + 1) * 128]


def home_kernel(cap, home_ref, code_ref, part_ref, tok_out_ref, router_ref):
    share = part_ref.shape[1]
    code = code_ref[...]
    n_tok, experts = code.shape
    rows = experts * cap
    code_of = mm(code.astype(BF16), spread(experts, cap).astype(BF16), NT)
    pick = code_of == ((iota((n_tok, rows), 1) & (cap - 1)) + 1).astype(F32)
    flat = home_ref[...].reshape(rows, home_ref.shape[2])
    tok_out_ref[...] = (
        mm(pick.astype(F32).astype(BF16), flat[:, :share], NN) + part_ref[...]
    ).astype(BF16)
    both = jnp.sum(home_ref[:, :, share:].astype(F32), axis=0)
    pieces = share // 128
    router_ref[...] = both[:pieces] + both[pieces:]


def cost(flops, data):
    return pl.CostEstimate(flops=flops, bytes_accessed=data, transcendentals=0)


def call(body, outs, n_in, flops, scalar=True, hbm=0, scratch=(), own=None):
    ins = ([SMEM] if scalar else []) + [VMEM] * n_in + [pl.BlockSpec(memory_space=pl.ANY)] * hbm
    if own is not None:
        dims, at = own
        ins[1] = pl.BlockSpec(dims, lambda i: (at, 0))
    return pl.pallas_call(
        body,
        out_shape=outs,
        grid=(1,),
        in_specs=ins,
        out_specs=[VMEM] * len(outs),
        scratch_shapes=list(scratch),
        cost_estimate=cost(flops, 4 << 20),
    )


def shape(dims, dtype):
    return jax.ShapeDtypeStruct(dims, dtype)


def per_device(tokens, out_grad, expert_ids, router_weight, w_gate, w_up, w_down):
    n_tok, width = tokens.shape
    experts = router_weight.shape[1]
    peers = lax.axis_size("ep")
    tp = lax.axis_size("tp")
    cap = 8
    share = width // tp
    ff = w_gate.shape[2]
    rows = peers * cap
    half = rows // 2
    me = jnp.full((1,), lax.axis_index("tp"), jnp.int32)
    unit = 2 * rows * share * ff
    router_t = router_weight.T

    def hop(value, by):
        return lax.ppermute(value, "tp", [(i, (i + by) % tp) for i in range(tp)])

    def exchange(value):
        return lax.all_to_all(value, "ep", split_axis=0, concat_axis=0, tiled=True)

    send, code, gate = call(
        functools.partial(dispatch_kernel, cap),
        [shape((rows, 2 * share), BF16), shape((n_tok, experts), F32), shape((n_tok, experts), F32)],
        4,
        unit,
    )(me, tokens, out_grad, expert_ids.T, router_t)
    own = exchange(send.reshape(peers, cap, 2 * share)).reshape(rows, 2 * share)
    piece = half // 2
    own1a, own1b = own[half : half + piece], own[half + piece :]
    p0, n0 = hop(own[:half], 1), hop(own[:half], -1)
    p1a, n1a = hop(own1a, 1), hop(own1b, -1)
    f0a, f0b = hop(p0[:piece], 1), hop(n0[piece:], -1)
    p1b, n1b = hop(own1b, 1), hop(own1a, -1)
    f1a, f1b = hop(p1a, 1), hop(n1a, -1)
    wg, wu, wd = w_gate[0], w_up[0], w_down[0]
    w_scratch = [pltpu.VMEM((width, ff), BF16), pltpu.VMEM((width, ff), BF16), pltpu.VMEM((ff, width), BF16)]

    def sems(n):
        return [pltpu.SemaphoreType.DMA((n,))]

    grads = [shape((half, ff), BF16)] * 3
    parts = (
        [shape((half, share), BF16)] * 2 + [shape((piece, share), F32)] * 2 + [shape((half, share), F32)]
    )
    hid0, dg0, du0, score0, *parts0 = call(
        functools.partial(first_kernel, cap),
        grads + [shape((half // cap, 128), F32)] + parts,
        5,
        10 * unit,
        hbm=3,
        scratch=w_scratch + sems(12),
        own=((half, 2 * share), 0),
    )(me, own, p0, n0, f0a, f0b, wg, wu, wd)
    near = call(
        near_kernel,
        [shape((half, ff), F32)] * 3,
        5,
        5 * unit,
        hbm=3,
        scratch=w_scratch + sems(9),
        own=((half, 2 * share), 1),
    )(me, own, p1a, p1b, n1a, n1b, wg, wu, wd)
    hid1, dg1, du1, score = call(
        functools.partial(far_kernel, cap),
        grads + [shape((peers, 128), F32)],
        6,
        3 * unit,
        hbm=3,
        scratch=w_scratch + sems(3),
    )(me, f1a, f1b, *near, score0, wg, wu, wd)
    parts1 = call(token_kernel, parts, 2, 4 * unit, hbm=2, scratch=w_scratch[:2] + sems(8))(me, dg1, du1, wg, wu)

    def summed(plus, minus, b1, b3, b0):
        rp, rm = hop(plus, 1), hop(minus, -1)
        ep = hop((b1 + rp[:piece].astype(F32)).astype(BF16), 1)
        em = hop((b3 + rm[piece:].astype(F32)).astype(BF16), -1)
        return b0, rp, rm, ep, em

    sums = summed(*parts0) + summed(*parts1)
    score = score + hop(score, 1) + hop(score, -1) + hop(score, 2)
    q = exchange(score.reshape(peers, 1, 128)).reshape(peers, 128)
    payload, d_logits = call(
        functools.partial(router_kernel, cap),
        [shape((peers, cap, share + 128), BF16), shape((n_tok, experts), F32)],
        14,
        unit,
    )(me, q, code, gate, tokens, *sums)
    home = exchange(payload)
    gwg, gwu, gwd, part = call(
        weight_kernel,
        [shape((width, ff), BF16), shape((width, ff), BF16), shape((ff, width), BF16), shape((n_tok, share), F32)],
        19,
        12 * unit,
    )(me, own, p0, p1a, p1b, n0, n1a, n1b, f0a, f0b, f1a, f1b, hid0, hid1, dg0, dg1, du0, du1, d_logits, router_t)
    token_grad, router = call(
        functools.partial(home_kernel, cap),
        [shape((n_tok, share), BF16), shape((share // 128, 128), F32)],
        3,
        unit,
        scalar=False,
    )(home, code, part)
    return (token_grad, router.reshape(share, 1), gwg[None], gwu[None], gwd[None])


def solution(mesh):
    in_specs = (
        P("ep", None),
        P("ep", None),
        P("ep", None),
        P(),
        P("ep", None, "tp"),
        P("ep", None, "tp"),
        P("ep", "tp", None),
    )
    out_specs = (
        P("ep", "tp"),
        P("tp", "ep"),
        P("ep", None, "tp"),
        P("ep", None, "tp"),
        P("ep", "tp", None),
    )

    return jax.shard_map(per_device, mesh=mesh, in_specs=in_specs, out_specs=out_specs, check_vma=False)
```

```python
import functools

import jax
import jax.numpy as jnp
from jax import lax
from jax.experimental import pallas as pl
from jax.experimental.pallas import tpu as pltpu
from jax.sharding import PartitionSpec as P


F32 = jnp.float32
BF16 = jnp.bfloat16
HI = lax.Precision.HIGHEST
VMEM = pl.BlockSpec(memory_space=pltpu.VMEM)
SMEM = pl.BlockSpec(memory_space=pltpu.SMEM)


def mm(a, b, dims, precision=None):
    return lax.dot_general(a, b, (dims, ((), ())), precision=precision, preferred_element_type=F32)


NN = ((1,), (0,))
NT = ((1,), (1,))
TN = ((0,), (0,))


def iota(shape, dim):
    return lax.broadcasted_iota(jnp.int32, shape, dim)


def bits(cap):
    return cap.bit_length() - 1


def spread(experts, cap):
    rows = experts * cap
    return ((iota((rows, experts), 0) >> bits(cap)) == iota((rows, experts), 1)).astype(F32)


def dispatch_kernel(cap, tp_ref, tok_ref, og_ref, ids_ref, rw_ref, send_ref, code_ref, gate_ref, mine_ref):
    n_tok = tok_ref.shape[0]
    experts = rw_ref.shape[0]
    share = send_ref.shape[1] // 2
    start = pl.multiple_of(tp_ref[0] * share, share)
    logits = mm(tok_ref[...], rw_ref[...], NT)
    ids = ids_ref[...].astype(F32).T
    lane = iota((n_tok, experts), 1).astype(F32)
    hit = lane == ids[:, 0:1]
    for k in range(1, ids.shape[1]):
        hit = hit | (lane == ids[:, k : k + 1])
    mask = hit.astype(F32)
    top = jnp.max(jnp.where(hit, logits, -jnp.inf), axis=1, keepdims=True)
    weight = jnp.where(hit, jnp.exp(jnp.where(hit, logits - top, 0.0)), 0.0)
    gate = weight / jnp.sum(weight, axis=1, keepdims=True)
    earlier = (iota((n_tok, n_tok), 1) < iota((n_tok, n_tok), 0)).astype(BF16)
    rank = mm(earlier, mask.astype(BF16), NN)
    code = mask * (rank + 1.0)
    code_ref[...] = code
    gate_ref[...] = gate
    expand = spread(experts, cap).astype(BF16)
    rows = experts * cap
    code_of = mm(expand, code.astype(BF16), NT)
    pick = code_of == ((iota((rows, n_tok), 0) & (cap - 1)) + 1).astype(F32)
    gate_of, rest = None, gate
    for _ in range(3):
        piece = rest.astype(BF16)
        rest = rest - piece.astype(F32)
        term = mm(expand, piece, NT)
        gate_of = term if gate_of is None else gate_of + term
    gate_of = jnp.sum(jnp.where(pick, gate_of, 0.0), axis=1, keepdims=True)
    mine = tok_ref[:, pl.ds(start, share)]
    mine_ref[...] = mine
    both = mm(pick.astype(F32).astype(BF16), jnp.concatenate([mine, og_ref[:, pl.ds(start, share)]], axis=1), NN)
    send_ref[:, :share] = both[:, :share].astype(BF16)
    send_ref[:, share:] = (both[:, share:] * gate_of).astype(BF16)


LEFT, RIGHT = 0, 1


def joined(refs, side):
    share = refs[0].shape[1] // 2
    return jnp.concatenate([r[:, side * share : (side + 1) * share] for r in refs], axis=0)


def block(tp_ref, off, share):
    return pl.ds(pl.multiple_of(lax.rem(tp_ref[0] + off, 4) * share, share), share)


def forward(tp_ref, groups, share, wgu, wd, start=None):
    total = start
    for off, refs in groups:
        at = block(tp_ref, off, share)
        terms = (mm(joined(refs, LEFT), wgu[at, :], NN), mm(joined(refs, RIGHT), wd[:, at], NT))
        total = terms if total is None else tuple(a + b for a, b in zip(total, terms))
    return total


def units(cap, both_pre, back):
    rows, ff = back.shape
    gate_pre, up_pre = both_pre[:, :ff], both_pre[:, ff:]
    glu = jnp.minimum(gate_pre, 7.0)
    linear = jnp.clip(up_pre, -7.0, 7.0)
    sig = jax.nn.sigmoid(1.702 * glu)
    act = glu * sig
    hidden = (linear + 1.0) * act
    slope = (linear + 1.0) * (sig + 1.702 * glu * sig * (1.0 - sig))
    slope = jnp.where(gate_pre < 7.0, slope, 0.0)
    up_slope = jnp.where((up_pre > -7.0) & (up_pre < 7.0), act, 0.0)
    score = jnp.sum(hidden * back, axis=1, keepdims=True)
    peers = rows // cap
    spot = ((iota((rows, 128), 0) & (cap - 1)) == iota((rows, 128), 1)).astype(F32) * score
    group = ((iota((peers, rows), 1) >> bits(cap)) == iota((peers, rows), 0)).astype(F32)
    grads = jnp.concatenate([(back * slope).astype(BF16), (back * up_slope).astype(BF16)], axis=1)
    return hidden.astype(BF16), grads, mm(group, spot, NN, HI)


def token_parts(tp_ref, grads, wgu, outs):
    plus_ref, minus_ref, b0_ref, b1_ref, b3_ref = outs
    rows, share = b0_ref.shape
    half = rows // 2

    def part(off):
        return mm(grads, wgu[block(tp_ref, off, share), :], NT)

    far = part(2).astype(BF16)
    plus_ref[:half, :] = far[:half]
    minus_ref[half:, :] = far[half:]
    ahead = part(1)
    b1_ref[...] = ahead[:half]
    plus_ref[half:, :] = ahead[half:].astype(BF16)
    behind = part(3)
    minus_ref[:half, :] = behind[:half].astype(BF16)
    b3_ref[...] = behind[half:]
    b0_ref[...] = part(0)


def first_kernel(cap, tp_ref, own, p0, n0, f0a, f0b, wgu, wd, b1, b3, hid, grads, score, plus, minus, b0):
    groups = ((0, (own,)), (3, (p0,)), (1, (n0,)), (2, (f0a, f0b)))
    hid[...], values, score[...] = units(cap, *forward(tp_ref, groups, b0.shape[1], wgu, wd))
    grads[...] = values
    token_parts(tp_ref, values, wgu, (plus, minus, b0, b1, b3))


def near_kernel(tp_ref, own, p1a, p1b, n1a, n1b, wgu, wd, pre, bk):
    groups = ((0, (own,)), (3, (p1a, p1b)), (1, (n1b, n1a)))
    pre[...], bk[...] = forward(tp_ref, groups, own.shape[1] // 2, wgu, wd)


def far_kernel(cap, tp_ref, f1a, f1b, pre, bk, score0, wgu, wd, hid, grads, score):
    start = (pre[...], bk[...])
    share = f1a.shape[1] // 2
    hid[...], grads[...], mine = units(cap, *forward(tp_ref, ((2, (f1a, f1b)),), share, wgu, wd, start))
    score[...] = jnp.concatenate([score0[...], mine], axis=0)


def token_kernel(tp_ref, grads, wgu, b1, b3, plus, minus, b0):
    token_parts(tp_ref, grads[...], wgu, (plus, minus, b0, b1, b3))


def weight_kernel(tp_ref, own, p0, p1a, p1b, n0, n1a, n1b, f0a, f0b, f1a, f1b, hid0, hid1, grads0, grads1,
                  d_logits_ref, rw_ref, gwg_ref, gwu_ref, gwd_ref, part_ref):
    share = own.shape[1] // 2
    ff = gwg_ref.shape[1]
    part_ref[...] = mm(d_logits_ref[...], rw_ref[:, block(tp_ref, 0, share)].astype(F32), NN, HI)
    hid = jnp.concatenate([hid0[...], hid1[...]], axis=0)
    grads = jnp.concatenate([grads0[...], grads1[...]], axis=0)
    for off, refs in ((0, (own,)), (3, (p0, p1a, p1b)), (1, (n0, n1b, n1a)), (2, (f0a, f0b, f1a, f1b))):
        at = block(tp_ref, off, share)
        t, g = joined(refs, LEFT), joined(refs, RIGHT)
        both = mm(t, grads, TN).astype(BF16)
        gwg_ref[at, :] = both[:, :ff]
        gwu_ref[at, :] = both[:, ff:]
        gwd_ref[:, at] = mm(hid, g, TN).astype(BF16)


def router_kernel(cap, q_ref, code_ref, gate_ref, tok_ref, *refs):
    sums, (payload_ref, d_logits_ref) = refs[:10], refs[10:]
    share = sums[0].shape[1]
    for h in range(2):
        b0, rp, rm, ep, em = sums[5 * h : 5 * h + 5]
        half = b0.shape[0] // 2
        top = b0[:half] + ep[...].astype(F32) + rm[:half].astype(F32)
        low = b0[half:] + rp[half:].astype(F32) + em[...].astype(F32)
        for i, value in enumerate((top, low)):
            n = half // cap
            at = pl.ds((2 * h + i) * n, n)
            payload_ref[at, :, :share] = value.astype(BF16).reshape(n, cap, share)
    code, gate = code_ref[...], gate_ref[...]
    q = q_ref[...].T
    score = jnp.zeros_like(code)
    for r in range(cap):
        score = score + jnp.where(code == r + 1.0, q[r : r + 1, :], 0.0)
    d_logits = score - gate * jnp.sum(score, axis=1, keepdims=True)
    d_logits_ref[...] = d_logits
    term = mm(d_logits, tok_ref[...].astype(F32), TN, HI)
    high = term.astype(BF16)
    low = (term - high.astype(F32)).astype(BF16)
    pieces = share // 128
    for j in range(pieces):
        payload_ref[:, j, share:] = high[:, j * 128 : (j + 1) * 128]
        payload_ref[:, pieces + j, share:] = low[:, j * 128 : (j + 1) * 128]


def home_kernel(cap, home_ref, code_ref, part_ref, tok_out_ref, router_ref):
    share = part_ref.shape[1]
    code = code_ref[...]
    n_tok, experts = code.shape
    rows = experts * cap
    code_of = mm(code.astype(BF16), spread(experts, cap).astype(BF16), NT)
    pick = code_of == ((iota((n_tok, rows), 1) & (cap - 1)) + 1).astype(F32)
    flat = home_ref[...].reshape(rows, home_ref.shape[2])
    tok_out_ref[...] = (
        mm(pick.astype(F32).astype(BF16), flat[:, :share], NN) + part_ref[...]
    ).astype(BF16)
    both = jnp.sum(home_ref[:, :, share:].astype(F32), axis=0)
    pieces = share // 128
    router_ref[...] = both[:pieces] + both[pieces:]


def cost(flops, data):
    return pl.CostEstimate(flops=flops, bytes_accessed=data, transcendentals=0)


def call(body, outs, flops, scalar=True, to_hbm=0, raw=()):
    def place(i, x):
        return pltpu.with_memory_space_constraint(x, pltpu.HBM if i in raw else pltpu.VMEM)

    def run(*args):
        ins = args[1:] if scalar else args
        return pl.pallas_call(
            body,
            out_shape=outs[:to_hbm] + [pltpu.VMEM(o.shape, o.dtype) for o in outs[to_hbm:]],
            in_specs=([SMEM] if scalar else []) + [VMEM] * len(ins),
            out_specs=[VMEM] * len(outs),
            cost_estimate=cost(flops, 4 << 20),
            compiler_params=pltpu.CompilerParams(vmem_limit_bytes=24 << 20),
        )(*args[: len(args) - len(ins)], *(place(i, x) for i, x in enumerate(ins)))

    return run


def shape(dims, dtype):
    return jax.ShapeDtypeStruct(dims, dtype)


def per_device(tokens, out_grad, expert_ids, router_weight, w_gate, w_up, w_down):
    n_tok, width = tokens.shape
    experts = router_weight.shape[1]
    peers = lax.axis_size("ep")
    tp = lax.axis_size("tp")
    cap = 8
    share = width // tp
    ff = w_gate.shape[2]
    rows = peers * cap
    half = rows // 2
    me = jnp.full((1,), lax.axis_index("tp"), jnp.int32)
    unit = 2 * rows * share * ff
    router_t = router_weight.T

    def hop(value, by):
        return lax.ppermute(value, "tp", [(i, (i + by) % tp) for i in range(tp)])

    def exchange(value):
        return lax.all_to_all(value, "ep", split_axis=0, concat_axis=0, tiled=True)

    send, code, gate, mine = call(
        functools.partial(dispatch_kernel, cap),
        [shape((rows, 2 * share), BF16), shape((n_tok, experts), F32), shape((n_tok, experts), F32),
         shape((n_tok, share), BF16)],
        unit,
        raw=(0, 1, 2, 3),
    )(me, tokens, out_grad, expert_ids.T, router_t)
    own = exchange(send.reshape(peers, cap, 2 * share)).reshape(rows, 2 * share)
    piece = half // 2
    own1a, own1b = own[half : half + piece], own[half + piece :]
    p0, n0 = hop(own[:half], 1), hop(own[:half], -1)
    p1a, n1a = hop(own1a, 1), hop(own1b, -1)
    f0a, f0b = hop(p0[:piece], 1), hop(n0[piece:], -1)
    p1b, n1b = hop(own1b, 1), hop(own1a, -1)
    f1a, f1b = hop(p1a, 1), hop(n1a, -1)

    def load_kernel(wg, wu, wd, wgu_out, wd_out, sems):
        copies = [
            pltpu.make_async_copy(wg, wgu_out.at[:, :ff], sems.at[0]),
            pltpu.make_async_copy(wu, wgu_out.at[:, ff:], sems.at[1]),
            pltpu.make_async_copy(wd, wd_out, sems.at[2]),
        ]
        for copy in copies:
            copy.start()
        for copy in copies:
            copy.wait()

    wgu, wd = pl.pallas_call(
        load_kernel,
        out_shape=[pltpu.VMEM((width, 2 * ff), BF16), pltpu.VMEM((ff, width), BF16)],
        in_specs=[pl.BlockSpec(memory_space=pl.ANY)] * 3,
        out_specs=[VMEM] * 2,
        scratch_shapes=[pltpu.SemaphoreType.DMA((3,))],
        cost_estimate=cost(unit, 4 << 20),
        compiler_params=pltpu.CompilerParams(vmem_limit_bytes=24 << 20),
    )(*(pltpu.with_memory_space_constraint(w[0], pltpu.HBM) for w in (w_gate, w_up, w_down)))

    grads = [shape((half, ff), BF16), shape((half, 2 * ff), BF16)]
    kept = [shape((piece, share), F32)] * 2
    parts = [shape((half, share), BF16)] * 2 + [shape((half, share), F32)]
    b10, b30, hid0, grads0, score0, plus0, minus0, b00 = call(
        functools.partial(first_kernel, cap),
        kept + grads + [shape((half // cap, 128), F32)] + parts,
        10 * unit,
        to_hbm=2,
    )(me, own[:half], p0, n0, f0a, f0b, wgu, wd)
    near = call(
        near_kernel, [shape((half, 2 * ff), F32), shape((half, ff), F32)], 5 * unit
    )(me, own[half:], p1a, p1b, n1a, n1b, wgu, wd)
    hid1, grads1, score = call(
        functools.partial(far_kernel, cap), grads + [shape((peers, 128), F32)], 3 * unit
    )(me, f1a, f1b, *near, score0, wgu, wd)
    b11, b31, plus1, minus1, b01 = call(token_kernel, kept + parts, 4 * unit, to_hbm=2)(me, grads1, wgu)

    def summed(plus, minus, b1, b3, b0):
        rp, rm = hop(plus, 1), hop(minus, -1)
        ep = hop((b1 + rp[:piece].astype(F32)).astype(BF16), 1)
        em = hop((b3 + rm[piece:].astype(F32)).astype(BF16), -1)
        return b0, rp, rm, ep, em

    sums = summed(plus0, minus0, b10, b30, b00) + summed(plus1, minus1, b11, b31, b01)
    score = score + hop(score, 1) + hop(score, -1) + hop(score, 2)
    q = exchange(score.reshape(peers, 1, 128)).reshape(peers, 128)
    payload, d_logits = call(
        functools.partial(router_kernel, cap),
        [shape((peers, cap, share + 128), BF16), shape((n_tok, experts), F32)],
        unit,
        scalar=False,
    )(q, code, gate, mine, *sums)
    home = exchange(payload)
    gwg, gwu, gwd, part = call(
        weight_kernel,
        [shape((width, ff), BF16), shape((width, ff), BF16), shape((ff, width), BF16), shape((n_tok, share), F32)],
        12 * unit,
        to_hbm=3,
        raw=range(17),
    )(me, own, p0, p1a, p1b, n0, n1a, n1b, f0a, f0b, f1a, f1b, hid0, hid1, grads0, grads1, d_logits, router_t)
    token_grad, router = call(
        functools.partial(home_kernel, cap),
        [shape((n_tok, share), BF16), shape((share // 128, 128), F32)],
        unit,
        to_hbm=2,
        scalar=False,
    )(home, code, part)
    return (token_grad, router.reshape(share, 1), gwg[None], gwu[None], gwd[None])


def solution(mesh):
    in_specs = (
        P("ep", None),
        P("ep", None),
        P("ep", None),
        P(),
        P("ep", None, "tp"),
        P("ep", None, "tp"),
        P("ep", "tp", None),
    )
    out_specs = (
        P("ep", "tp"),
        P("tp", "ep"),
        P("ep", None, "tp"),
        P("ep", None, "tp"),
        P("ep", "tp", None),
    )

    return jax.shard_map(per_device, mesh=mesh, in_specs=in_specs, out_specs=out_specs, check_vma=False)
```

```python
import functools

import jax
import jax.numpy as jnp
from jax import lax
from jax.experimental import pallas as pl
from jax.experimental.pallas import tpu as pltpu
from jax.sharding import PartitionSpec as P


F32 = jnp.float32
BF16 = jnp.bfloat16
HI = lax.Precision.HIGHEST
VMEM = pl.BlockSpec(memory_space=pltpu.VMEM)
SMEM = pl.BlockSpec(memory_space=pltpu.SMEM)


def mm(a, b, dims, precision=None):
    return lax.dot_general(a, b, (dims, ((), ())), precision=precision, preferred_element_type=F32)


NN = ((1,), (0,))
NT = ((1,), (1,))
TN = ((0,), (0,))


def iota(shape, dim):
    return lax.broadcasted_iota(jnp.int32, shape, dim)


def bits(cap):
    return cap.bit_length() - 1


def spread(experts, cap):
    rows = experts * cap
    return ((iota((rows, experts), 0) >> bits(cap)) == iota((rows, experts), 1)).astype(F32)


def dispatch_kernel(cap, tp_ref, tok_ref, og_ref, ids_ref, rw_ref, send_ref, code_ref, gate_ref, mine_ref):
    n_tok = tok_ref.shape[0]
    experts = rw_ref.shape[0]
    share = send_ref.shape[1] // 2
    start = pl.multiple_of(tp_ref[0] * share, share)
    logits = mm(tok_ref[...], rw_ref[...], NT)
    ids = ids_ref[...].astype(F32).T
    lane = iota((n_tok, experts), 1).astype(F32)
    hit = lane == ids[:, 0:1]
    for k in range(1, ids.shape[1]):
        hit = hit | (lane == ids[:, k : k + 1])
    mask = hit.astype(F32)
    top = jnp.max(jnp.where(hit, logits, -jnp.inf), axis=1, keepdims=True)
    weight = jnp.where(hit, jnp.exp(jnp.where(hit, logits - top, 0.0)), 0.0)
    gate = weight / jnp.sum(weight, axis=1, keepdims=True)
    earlier = (iota((n_tok, n_tok), 1) < iota((n_tok, n_tok), 0)).astype(BF16)
    rank = mm(earlier, mask.astype(BF16), NN)
    code = mask * (rank + 1.0)
    code_ref[...] = code
    gate_ref[...] = gate
    expand = spread(experts, cap).astype(BF16)
    rows = experts * cap
    code_of = mm(expand, code.astype(BF16), NT)
    pick = code_of == ((iota((rows, n_tok), 0) & (cap - 1)) + 1).astype(F32)
    gate_of, rest = None, gate
    for _ in range(3):
        piece = rest.astype(BF16)
        rest = rest - piece.astype(F32)
        term = mm(expand, piece, NT)
        gate_of = term if gate_of is None else gate_of + term
    gate_of = jnp.sum(jnp.where(pick, gate_of, 0.0), axis=1, keepdims=True)
    mine = tok_ref[:, pl.ds(start, share)]
    mine_ref[...] = mine
    both = mm(pick.astype(F32).astype(BF16), jnp.concatenate([mine, og_ref[:, pl.ds(start, share)]], axis=1), NN)
    send_ref[:, :share] = both[:, :share].astype(BF16)
    send_ref[:, share:] = (both[:, share:] * gate_of).astype(BF16)


LEFT, RIGHT = 0, 1


def joined(refs, side):
    share = refs[0].shape[1] // 2
    return jnp.concatenate([r[:, side * share : (side + 1) * share] for r in refs], axis=0)


def block(tp_ref, off, share):
    return pl.ds(pl.multiple_of(lax.rem(tp_ref[0] + off, 4) * share, share), share)


def forward(tp_ref, groups, share, wgu, wd, start=None):
    total = start
    for off, refs in groups:
        at = block(tp_ref, off, share)
        terms = (mm(joined(refs, LEFT), wgu[at, :], NN), mm(joined(refs, RIGHT), wd[:, at], NT))
        total = terms if total is None else tuple(a + b for a, b in zip(total, terms))
    return total


def units(cap, both_pre, back):
    rows, ff = back.shape
    gate_pre, up_pre = both_pre[:, :ff], both_pre[:, ff:]
    glu = jnp.minimum(gate_pre, 7.0)
    linear = jnp.clip(up_pre, -7.0, 7.0)
    sig = jax.nn.sigmoid(1.702 * glu)
    act = glu * sig
    hidden = (linear + 1.0) * act
    slope = (linear + 1.0) * (sig + 1.702 * glu * sig * (1.0 - sig))
    slope = jnp.where(gate_pre < 7.0, slope, 0.0)
    up_slope = jnp.where((up_pre > -7.0) & (up_pre < 7.0), act, 0.0)
    score = jnp.sum(hidden * back, axis=1, keepdims=True)
    peers = rows // cap
    spot = ((iota((rows, 128), 0) & (cap - 1)) == iota((rows, 128), 1)).astype(F32) * score
    group = ((iota((peers, rows), 1) >> bits(cap)) == iota((peers, rows), 0)).astype(F32)
    grads = jnp.concatenate([(back * slope).astype(BF16), (back * up_slope).astype(BF16)], axis=1)
    return hidden.astype(BF16), grads, mm(group, spot, NN, HI)


def near_kernel(tp_ref, own, pa, pb, na, nb, wgu, wd, pre, bk):
    groups = ((0, (own,)), (3, (pa, pb)), (1, (na, nb)))
    pre[...], bk[...] = forward(tp_ref, groups, own.shape[1] // 2, wgu, wd)


def far_kernel(cap, tp_ref, f0, f1, pre, bk, wgu, wd, hid, grads, score, b2a, b2b):
    share = f0.shape[1] // 2
    half = f0.shape[0]
    start = (pre[...], bk[...])
    hid[...], values, score[...] = units(cap, *forward(tp_ref, ((2, (f0, f1)),), share, wgu, wd, start))
    grads[...] = values
    far = mm(values, wgu[block(tp_ref, 2, share), :], NT).astype(BF16)
    b2a[...] = far[:half]
    b2b[...] = far[half:]


def token_kernel(tp_ref, grads_ref, wgu, b1a, b1b, b3a, b3b, b0):
    share = b0.shape[1]
    half = b0.shape[0] // 2
    grads = grads_ref[...]

    def part(off):
        return mm(grads, wgu[block(tp_ref, off, share), :], NT)

    ahead = part(1)
    b1a[...] = ahead[:half]
    b1b[...] = ahead[half:].astype(BF16)
    behind = part(3)
    b3a[...] = behind[:half].astype(BF16)
    b3b[...] = behind[half:]
    b0[...] = part(0)


def total_kernel(a, b, c, d, out):
    out[...] = a[...] + b[...] + c[...] + d[...]


def onward_kernel(b1a, s1, b3b, s2, ahead, behind):
    ahead[...] = (b1a[...] + s1[...].astype(F32)).astype(BF16)
    behind[...] = (b3b[...] + s2[...].astype(F32)).astype(BF16)


def weight_kernel(tp_ref, own, pa, pb, na, nb, f0, f1, hid, grads, d_logits_ref, rw_ref,
                  gwg_ref, gwu_ref, gwd_ref, part_ref):
    share = own.shape[1] // 2
    ff = gwg_ref.shape[1]
    part_ref[...] = mm(d_logits_ref[...], rw_ref[:, block(tp_ref, 0, share)].astype(F32), NN, HI)
    for off, refs in ((0, (own,)), (3, (pa, pb)), (1, (na, nb)), (2, (f0, f1))):
        at = block(tp_ref, off, share)
        t, g = joined(refs, LEFT), joined(refs, RIGHT)
        both = mm(t, grads[...], TN).astype(BF16)
        gwg_ref[at, :] = both[:, :ff]
        gwu_ref[at, :] = both[:, ff:]
        gwd_ref[:, at] = mm(hid[...], g, TN).astype(BF16)


def router_kernel(cap, q_ref, code_ref, gate_ref, tok_ref, *refs):
    (b0, d1, d2, e1, e2), (payload_ref, d_logits_ref) = refs[:5], refs[5:]
    rows, share = b0.shape
    half = rows // 2
    for i, (near, far) in enumerate(((d2, e1), (d1, e2))):
        n = half // cap
        value = b0[i * half : (i + 1) * half] + near[...].astype(F32) + far[...].astype(F32)
        payload_ref[pl.ds(i * n, n), :, :share] = value.astype(BF16).reshape(n, cap, share)
    code, gate = code_ref[...], gate_ref[...]
    q = q_ref[...].T
    score = jnp.zeros_like(code)
    for r in range(cap):
        score = score + jnp.where(code == r + 1.0, q[r : r + 1, :], 0.0)
    d_logits = score - gate * jnp.sum(score, axis=1, keepdims=True)
    d_logits_ref[...] = d_logits
    term = mm(d_logits, tok_ref[...].astype(F32), TN, HI)
    high = term.astype(BF16)
    low = (term - high.astype(F32)).astype(BF16)
    pieces = share // 128
    for j in range(pieces):
        payload_ref[:, j, share:] = high[:, j * 128 : (j + 1) * 128]
        payload_ref[:, pieces + j, share:] = low[:, j * 128 : (j + 1) * 128]


def mark_kernel(given, out):
    out[...] = given[...]


def home_kernel(cap, home_ref, code_ref, part_ref, tok_out_ref, router_ref):
    share = part_ref.shape[1]
    code = code_ref[...]
    n_tok, experts = code.shape
    rows = experts * cap
    code_of = mm(code.astype(BF16), spread(experts, cap).astype(BF16), NT)
    pick = code_of == ((iota((n_tok, rows), 1) & (cap - 1)) + 1).astype(F32)
    flat = home_ref[...].reshape(rows, home_ref.shape[2])
    tok_out_ref[...] = (
        mm(pick.astype(F32).astype(BF16), flat[:, :share], NN) + part_ref[...]
    ).astype(BF16)
    both = jnp.sum(home_ref[:, :, share:].astype(F32), axis=0)
    pieces = share // 128
    router_ref[...] = both[:pieces] + both[pieces:]


def cost(flops, data):
    return pl.CostEstimate(flops=flops, bytes_accessed=data, transcendentals=0)


def call(body, outs, flops, scalar=True, to_hbm=0, raw=()):
    def place(i, x):
        return pltpu.with_memory_space_constraint(x, pltpu.HBM if i in raw else pltpu.VMEM)

    def run(*args):
        ins = args[1:] if scalar else args
        return pl.pallas_call(
            body,
            out_shape=outs[:to_hbm] + [pltpu.VMEM(o.shape, o.dtype) for o in outs[to_hbm:]],
            in_specs=([SMEM] if scalar else []) + [VMEM] * len(ins),
            out_specs=[VMEM] * len(outs),
            cost_estimate=cost(flops, 4 << 20),
            compiler_params=pltpu.CompilerParams(vmem_limit_bytes=24 << 20),
        )(*args[: len(args) - len(ins)], *(place(i, x) for i, x in enumerate(ins)))

    return run


def shape(dims, dtype):
    return jax.ShapeDtypeStruct(dims, dtype)


def per_device(tokens, out_grad, expert_ids, router_weight, w_gate, w_up, w_down):
    n_tok, width = tokens.shape
    experts = router_weight.shape[1]
    peers = lax.axis_size("ep")
    tp = lax.axis_size("tp")
    cap = 8
    share = width // tp
    ff = w_gate.shape[2]
    rows = peers * cap
    half = rows // 2
    me = jnp.full((1,), lax.axis_index("tp"), jnp.int32)
    unit = 2 * rows * share * ff
    router_t = router_weight.T

    def hop(value, by):
        return lax.ppermute(value, "tp", [(i, (i + by) % tp) for i in range(tp)])

    def exchange(value):
        return lax.all_to_all(value, "ep", split_axis=0, concat_axis=0, tiled=True)

    send, code, gate, mine = call(
        functools.partial(dispatch_kernel, cap),
        [shape((rows, 2 * share), BF16), shape((n_tok, experts), F32), shape((n_tok, experts), F32),
         shape((n_tok, share), BF16)],
        unit,
        raw=(0, 1, 2, 3),
    )(me, tokens, out_grad, expert_ids.T, router_t)
    own = exchange(send.reshape(peers, cap, 2 * share)).reshape(rows, 2 * share)
    pa, nb = hop(own[:half], 1), hop(own[half:], -1)
    pb, na = hop(own[half:], 1), hop(own[:half], -1)
    f0, f1 = hop(pa, 1), hop(nb, -1)

    def load_kernel(wg, wu, wd, wgu_out, wd_out, sems):
        copies = [
            pltpu.make_async_copy(wg, wgu_out.at[:, :ff], sems.at[0]),
            pltpu.make_async_copy(wu, wgu_out.at[:, ff:], sems.at[1]),
            pltpu.make_async_copy(wd, wd_out, sems.at[2]),
        ]
        for copy in copies:
            copy.start()
        for copy in copies:
            copy.wait()

    wgu, wd = pl.pallas_call(
        load_kernel,
        out_shape=[pltpu.VMEM((width, 2 * ff), BF16), pltpu.VMEM((ff, width), BF16)],
        in_specs=[pl.BlockSpec(memory_space=pl.ANY)] * 3,
        out_specs=[VMEM] * 2,
        scratch_shapes=[pltpu.SemaphoreType.DMA((3,))],
        cost_estimate=cost(unit, 4 << 20),
        compiler_params=pltpu.CompilerParams(vmem_limit_bytes=24 << 20),
    )(*(pltpu.with_memory_space_constraint(w[0], pltpu.HBM) for w in (w_gate, w_up, w_down)))

    near = call(
        near_kernel, [shape((rows, 2 * ff), F32), shape((rows, ff), F32)], 9 * unit
    )(me, own, pa, pb, na, nb, wgu, wd)
    hid, grads, score, b2a, b2b = call(
        functools.partial(far_kernel, cap),
        [shape((rows, ff), BF16), shape((rows, 2 * ff), BF16), shape((peers, 128), F32)]
        + [shape((half, share), BF16)] * 2,
        5 * unit,
    )(me, f0, f1, *near, wgu, wd)
    s1, s2 = hop(b2a, 1), hop(b2b, -1)
    b1a, b1b, b3a, b3b, b0 = call(
        token_kernel,
        [shape((half, share), F32), shape((half, share), BF16), shape((half, share), BF16),
         shape((half, share), F32), shape((rows, share), F32)],
        6 * unit,
    )(me, grads, wgu)
    d1, d2 = hop(b1b, 1), hop(b3a, -1)
    ahead, behind = call(onward_kernel, [shape((half, share), BF16)] * 2, 1, scalar=False)(b1a, s1, b3b, s2)
    e1, e2 = hop(ahead, 1), hop(behind, -1)
    (gate,) = call(mark_kernel, [shape((n_tok, experts), F32)], 1, scalar=False)(gate)
    (score,) = call(total_kernel, [shape((peers, 128), F32)], 1, scalar=False)(
        score, hop(score, 1), hop(score, -1), hop(score, 2)
    )
    q = exchange(score.reshape(peers, 1, 128)).reshape(peers, 128)
    payload, d_logits = call(
        functools.partial(router_kernel, cap),
        [shape((peers, cap, share + 128), BF16), shape((n_tok, experts), F32)],
        unit,
        scalar=False,
    )(q, code, gate, mine, b0, d1, d2, e1, e2)
    home = exchange(payload)
    gwg, gwu, gwd, part = call(
        weight_kernel,
        [shape((width, ff), BF16), shape((width, ff), BF16), shape((ff, width), BF16), shape((n_tok, share), F32)],
        12 * unit,
        to_hbm=3,
        raw=range(11),
    )(me, own, pa, pb, na, nb, f0, f1, hid, grads, d_logits, router_t)
    token_grad, router = call(
        functools.partial(home_kernel, cap),
        [shape((n_tok, share), BF16), shape((share // 128, 128), F32)],
        unit,
        to_hbm=2,
        scalar=False,
    )(home, code, part)
    return (token_grad, router.reshape(share, 1), gwg[None], gwu[None], gwd[None])


def solution(mesh):
    in_specs = (
        P("ep", None),
        P("ep", None),
        P("ep", None),
        P(),
        P("ep", None, "tp"),
        P("ep", None, "tp"),
        P("ep", "tp", None),
    )
    out_specs = (
        P("ep", "tp"),
        P("tp", "ep"),
        P("ep", None, "tp"),
        P("ep", None, "tp"),
        P("ep", "tp", None),
    )

    return jax.shard_map(per_device, mesh=mesh, in_specs=in_specs, out_specs=out_specs, check_vma=False)
```

```python
import functools

import jax
import jax.numpy as jnp
from jax import lax
from jax.experimental import pallas as pl
from jax.experimental.pallas import tpu as pltpu
from jax.sharding import PartitionSpec as P


F32 = jnp.float32
BF16 = jnp.bfloat16
HI = lax.Precision.HIGHEST
VMEM = pl.BlockSpec(memory_space=pltpu.VMEM)
SMEM = pl.BlockSpec(memory_space=pltpu.SMEM)


def mm(a, b, dims, precision=None):
    return lax.dot_general(a, b, (dims, ((), ())), precision=precision, preferred_element_type=F32)


NN = ((1,), (0,))
NT = ((1,), (1,))
TN = ((0,), (0,))


def iota(shape, dim):
    return lax.broadcasted_iota(jnp.int32, shape, dim)


def bits(cap):
    return cap.bit_length() - 1


def spread(experts, cap):
    rows = experts * cap
    return ((iota((rows, experts), 0) >> bits(cap)) == iota((rows, experts), 1)).astype(F32)


def dispatch_kernel(cap, tp_ref, tok_ref, og_ref, ids_ref, rw_ref, send_ref, more_ref, code_ref, gate_ref, mine_ref):
    n_tok = tok_ref.shape[0]
    experts = rw_ref.shape[0]
    share = mine_ref.shape[1]
    start = pl.multiple_of(tp_ref[0] * share, share)
    logits = mm(tok_ref[...], rw_ref[...], NT)
    ids = ids_ref[...].astype(F32).T
    lane = iota((n_tok, experts), 1).astype(F32)
    hit = lane == ids[:, 0:1]
    for k in range(1, ids.shape[1]):
        hit = hit | (lane == ids[:, k : k + 1])
    mask = hit.astype(F32)
    top = jnp.max(jnp.where(hit, logits, -jnp.inf), axis=1, keepdims=True)
    weight = jnp.where(hit, jnp.exp(jnp.where(hit, logits - top, 0.0)), 0.0)
    gate = weight / jnp.sum(weight, axis=1, keepdims=True)
    earlier = (iota((n_tok, n_tok), 1) < iota((n_tok, n_tok), 0)).astype(BF16)
    rank = mm(earlier, mask.astype(BF16), NN)
    code = mask * (rank + 1.0)
    code_ref[...] = code
    gate_ref[...] = gate
    expand = spread(experts, cap).astype(BF16)
    rows = experts * cap
    code_of = mm(expand, code.astype(BF16), NT)
    pick = code_of == ((iota((rows, n_tok), 0) & (cap - 1)) + 1).astype(F32)
    gate_of, rest = None, gate
    for _ in range(3):
        piece = rest.astype(BF16)
        rest = rest - piece.astype(F32)
        term = mm(expand, piece, NT)
        gate_of = term if gate_of is None else gate_of + term
    gate_of = jnp.sum(jnp.where(pick, gate_of, 0.0), axis=1, keepdims=True)
    mine = tok_ref[:, pl.ds(start, share)]
    mine_ref[...] = mine
    relay = send_ref.shape[1] - share
    cots = [og_ref[:, pl.ds(start, relay)]]
    cots += [og_ref[:, j + relay : j + share] for j in range(0, og_ref.shape[1], share)]
    both = mm(pick.astype(F32).astype(BF16), jnp.concatenate([mine] + cots, axis=1), NN)
    send_ref[:, :share] = both[:, :share].astype(BF16)
    send_ref[:, share:] = (both[:, share : share + relay] * gate_of).astype(BF16)
    more_ref[...] = (both[:, share + relay :] * gate_of).astype(BF16)


def joined(refs, cols):
    return jnp.concatenate([r[:, cols] for r in refs], axis=0)


def block(tp_ref, off, share):
    return pl.ds(pl.multiple_of(lax.rem(tp_ref[0] + off, 4) * share, share), share)


def forward(tp_ref, groups, share, wgu, wd, start=None):
    total = start
    for off, refs in groups:
        at = block(tp_ref, off, share)
        relay = refs[0].shape[1] - share
        terms = (
            mm(joined(refs, slice(0, share)), wgu[at, :], NN),
            mm(joined(refs, slice(share, None)), wd[:, pl.ds(at.start, relay)], NT),
        )
        total = terms if total is None else tuple(a + b for a, b in zip(total, terms))
    return total


def units(cap, both_pre, back):
    rows, ff = back.shape
    gate_pre, up_pre = both_pre[:, :ff], both_pre[:, ff:]
    glu = jnp.minimum(gate_pre, 7.0)
    linear = jnp.clip(up_pre, -7.0, 7.0)
    sig = jax.nn.sigmoid(1.702 * glu)
    act = glu * sig
    hidden = (linear + 1.0) * act
    slope = (linear + 1.0) * (sig + 1.702 * glu * sig * (1.0 - sig))
    slope = jnp.where(gate_pre < 7.0, slope, 0.0)
    up_slope = jnp.where((up_pre > -7.0) & (up_pre < 7.0), act, 0.0)
    score = jnp.sum(hidden * back, axis=1, keepdims=True)
    peers = rows // cap
    spot = ((iota((rows, 128), 0) & (cap - 1)) == iota((rows, 128), 1)).astype(F32) * score
    group = ((iota((peers, rows), 1) >> bits(cap)) == iota((peers, rows), 0)).astype(F32)
    grads = jnp.concatenate([(back * slope).astype(BF16), (back * up_slope).astype(BF16)], axis=1)
    return hidden.astype(BF16), grads, mm(group, spot, NN, HI)


def near_kernel(share, tp_ref, own, pa, pb, na, nb, more, wgu, wd, pre, bk):
    groups = ((0, (own,)), (3, (pa, pb)), (1, (na, nb)))
    relay = own.shape[1] - share
    rest = jnp.concatenate([wd[:, j + relay : j + share] for j in range(0, wd.shape[1], share)], axis=1)
    pre[...], back = forward(tp_ref, groups, share, wgu, wd)
    bk[...] = back + mm(more[...], rest, NT)


def far_kernel(cap, tp_ref, f0, f1, pre, bk, wgu, wd, hid, grads, score, b2a, b2b):
    half, share = b2a.shape
    start = (pre[...], bk[...])
    hid[...], values, score[...] = units(cap, *forward(tp_ref, ((2, (f0, f1)),), share, wgu, wd, start))
    grads[...] = values
    far = mm(values, wgu[block(tp_ref, 2, share), :], NT).astype(BF16)
    b2a[...] = far[:half]
    b2b[...] = far[half:]


def token_kernel(tp_ref, grads_ref, wgu, b1a, b3b, b0, b1b, b3a):
    share = b0.shape[1]
    half = b0.shape[0] // 2
    grads = grads_ref[...]

    def part(off):
        return mm(grads, wgu[block(tp_ref, off, share), :], NT)

    ahead = part(1)
    b1a[...] = ahead[:half]
    b1b[...] = ahead[half:].astype(BF16)
    behind = part(3)
    b3a[...] = behind[:half].astype(BF16)
    b3b[...] = behind[half:]
    b0[...] = part(0)


def total_kernel(a, b, c, d, out):
    out[...] = a[...] + b[...] + c[...] + d[...]


def onward_kernel(b1a, s1, b3b, s2, ahead, behind):
    ahead[...] = (b1a[...] + s1[...].astype(F32)).astype(BF16)
    behind[...] = (b3b[...] + s2[...].astype(F32)).astype(BF16)


def weight_kernel(share, tp_ref, own, pa, pb, na, nb, f0, f1, more, hid, grads, d_logits_ref, rw_ref,
                  gwg_ref, gwu_ref, gwd_ref, part_ref):
    ff = gwg_ref.shape[1]
    relay = own.shape[1] - share
    part_ref[...] = mm(d_logits_ref[...], rw_ref[:, block(tp_ref, 0, share)].astype(F32), NN, HI)
    rest = mm(hid[...], more[...], TN).astype(BF16)
    for j in range(gwd_ref.shape[1] // share):
        gwd_ref[:, j * share + relay : (j + 1) * share] = rest[:, j * (share - relay) : (j + 1) * (share - relay)]
    for off, refs in ((0, (own,)), (3, (pa, pb)), (1, (na, nb)), (2, (f0, f1))):
        at = block(tp_ref, off, share)
        both = mm(joined(refs, slice(0, share)), grads[...], TN).astype(BF16)
        gwg_ref[at, :] = both[:, :ff]
        gwu_ref[at, :] = both[:, ff:]
        gwd_ref[:, pl.ds(at.start, relay)] = mm(hid[...], joined(refs, slice(share, None)), TN).astype(BF16)


def router_kernel(cap, q_ref, code_ref, gate_ref, tok_ref, *refs):
    (b0, d1, d2, e1, e2), (payload_ref, d_logits_ref) = refs[:5], refs[5:]
    rows, share = b0.shape
    half = rows // 2
    for i, (near, far) in enumerate(((d2, e1), (d1, e2))):
        n = half // cap
        value = b0[i * half : (i + 1) * half] + near[...].astype(F32) + far[...].astype(F32)
        payload_ref[pl.ds(i * n, n), :, :share] = value.astype(BF16).reshape(n, cap, share)
    code, gate = code_ref[...], gate_ref[...]
    q = q_ref[...].T
    score = jnp.zeros_like(code)
    for r in range(cap):
        score = score + jnp.where(code == r + 1.0, q[r : r + 1, :], 0.0)
    d_logits = score - gate * jnp.sum(score, axis=1, keepdims=True)
    d_logits_ref[...] = d_logits
    term = mm(d_logits, tok_ref[...].astype(F32), TN, HI)
    high = term.astype(BF16)
    low = (term - high.astype(F32)).astype(BF16)
    pieces = share // 128
    for j in range(pieces):
        payload_ref[:, j, share:] = high[:, j * 128 : (j + 1) * 128]
        payload_ref[:, pieces + j, share:] = low[:, j * 128 : (j + 1) * 128]


def mark_kernel(given, out):
    out[...] = given[...]


def home_kernel(cap, home_ref, code_ref, part_ref, tok_out_ref, router_ref):
    share = part_ref.shape[1]
    code = code_ref[...]
    n_tok, experts = code.shape
    rows = experts * cap
    code_of = mm(code.astype(BF16), spread(experts, cap).astype(BF16), NT)
    pick = code_of == ((iota((n_tok, rows), 1) & (cap - 1)) + 1).astype(F32)
    flat = home_ref[...].reshape(rows, home_ref.shape[2])
    tok_out_ref[...] = (
        mm(pick.astype(F32).astype(BF16), flat[:, :share], NN) + part_ref[...]
    ).astype(BF16)
    both = jnp.sum(home_ref[:, :, share:].astype(F32), axis=0)
    pieces = share // 128
    router_ref[...] = both[:pieces] + both[pieces:]


def cost(flops, data):
    return pl.CostEstimate(flops=flops, bytes_accessed=data, transcendentals=0)


def call(body, outs, flops, scalar=True, to_hbm=0, raw=()):
    def place(i, x):
        return pltpu.with_memory_space_constraint(x, pltpu.HBM if i in raw else pltpu.VMEM)

    def run(*args):
        ins = args[1:] if scalar else args
        return pl.pallas_call(
            body,
            out_shape=[(pltpu.HBM if i < to_hbm else pltpu.VMEM)(o.shape, o.dtype) for i, o in enumerate(outs)],
            in_specs=([SMEM] if scalar else []) + [VMEM] * len(ins),
            out_specs=[VMEM] * len(outs),
            cost_estimate=cost(flops, 4 << 20),
            compiler_params=pltpu.CompilerParams(vmem_limit_bytes=24 << 20),
        )(*args[: len(args) - len(ins)], *(place(i, x) for i, x in enumerate(ins)))

    return run


def shape(dims, dtype):
    return jax.ShapeDtypeStruct(dims, dtype)


def per_device(tokens, out_grad, expert_ids, router_weight, w_gate, w_up, w_down):
    n_tok, width = tokens.shape
    experts = router_weight.shape[1]
    peers = lax.axis_size("ep")
    tp = lax.axis_size("tp")
    cap = 8
    share = width // tp
    ff = w_gate.shape[2]
    rows = peers * cap
    half = rows // 2
    me = jnp.full((1,), lax.axis_index("tp"), jnp.int32)
    unit = 2 * rows * share * ff
    router_t = router_weight.T

    def hop(value, by):
        return lax.ppermute(value, "tp", [(i, (i + by) % tp) for i in range(tp)])

    def exchange(value):
        return lax.all_to_all(value, "ep", split_axis=0, concat_axis=0, tiled=True)

    relay = share - 128
    rest = tp * (share - relay)
    send, more, code, gate, mine = call(
        functools.partial(dispatch_kernel, cap),
        [shape((rows, share + relay), BF16), shape((rows, rest), BF16), shape((n_tok, experts), F32),
         shape((n_tok, experts), F32), shape((n_tok, share), BF16)],
        unit,
        raw=(0, 1, 2, 3),
    )(me, tokens, out_grad, expert_ids.T, router_t)
    own = exchange(send.reshape(peers, cap, share + relay)).reshape(rows, share + relay)
    more = exchange(more.reshape(peers, cap, rest)).reshape(rows, rest)
    pa, nb = hop(own[:half], 1), hop(own[half:], -1)
    pb, na = hop(own[half:], 1), hop(own[:half], -1)
    f0, f1 = hop(pa, 1), hop(nb, -1)

    def load_kernel(wg, wu, wd, wgu_out, wd_out, sems):
        copies = [
            pltpu.make_async_copy(wg, wgu_out.at[:, :ff], sems.at[0]),
            pltpu.make_async_copy(wu, wgu_out.at[:, ff:], sems.at[1]),
            pltpu.make_async_copy(wd, wd_out, sems.at[2]),
        ]
        for copy in copies:
            copy.start()
        for copy in copies:
            copy.wait()

    wgu, wd = pl.pallas_call(
        load_kernel,
        out_shape=[pltpu.VMEM((width, 2 * ff), BF16), pltpu.VMEM((ff, width), BF16)],
        in_specs=[pl.BlockSpec(memory_space=pl.ANY)] * 3,
        out_specs=[VMEM] * 2,
        scratch_shapes=[pltpu.SemaphoreType.DMA((3,))],
        cost_estimate=cost(unit, 4 << 20),
        compiler_params=pltpu.CompilerParams(vmem_limit_bytes=24 << 20),
    )(*(pltpu.with_memory_space_constraint(w[0], pltpu.HBM) for w in (w_gate, w_up, w_down)))

    near = call(
        functools.partial(near_kernel, share), [shape((rows, 2 * ff), F32), shape((rows, ff), F32)], 9 * unit
    )(me, own, pa, pb, na, nb, more, wgu, wd)
    hid, grads, score, b2a, b2b = call(
        functools.partial(far_kernel, cap),
        [shape((rows, ff), BF16), shape((rows, 2 * ff), BF16), shape((peers, 128), F32)]
        + [shape((half, share), BF16)] * 2,
        5 * unit,
    )(me, f0, f1, *near, wgu, wd)
    s1, s2 = hop(b2a, 1), hop(b2b, -1)
    b1a, b3b, b0, b1b, b3a = call(
        token_kernel,
        [shape((half, share), F32)] * 2 + [shape((rows, share), F32)] + [shape((half, share), BF16)] * 2,
        6 * unit,
        to_hbm=3,
    )(me, grads, wgu)
    d1, d2 = hop(b1b, 1), hop(b3a, -1)
    ahead, behind = call(onward_kernel, [shape((half, share), BF16)] * 2, 1, scalar=False, raw=(0, 2))(b1a, s1, b3b, s2)
    e1, e2 = hop(ahead, 1), hop(behind, -1)
    (gate,) = call(mark_kernel, [shape((n_tok, experts), F32)], 1, scalar=False)(gate)
    (score,) = call(total_kernel, [shape((peers, 128), F32)], 1, scalar=False)(
        score, hop(score, 1), hop(score, -1), hop(score, 2)
    )
    q = exchange(score.reshape(peers, 1, 128)).reshape(peers, 128)
    payload, d_logits = call(
        functools.partial(router_kernel, cap),
        [shape((peers, cap, share + 128), BF16), shape((n_tok, experts), F32)],
        unit,
        scalar=False,
        raw=(4,),
    )(q, code, gate, mine, b0, d1, d2, e1, e2)
    home = exchange(payload)
    gwg, gwu, gwd, part = call(
        functools.partial(weight_kernel, share),
        [shape((width, ff), BF16), shape((width, ff), BF16), shape((ff, width), BF16), shape((n_tok, share), F32)],
        12 * unit,
        to_hbm=3,
        raw=range(12),
    )(me, own, pa, pb, na, nb, f0, f1, more, hid, grads, d_logits, router_t)
    token_grad, router = call(
        functools.partial(home_kernel, cap),
        [shape((n_tok, share), BF16), shape((share // 128, 128), F32)],
        unit,
        to_hbm=2,
        scalar=False,
    )(home, code, part)
    return (token_grad, router.reshape(share, 1), gwg[None], gwu[None], gwd[None])


def solution(mesh):
    in_specs = (
        P("ep", None),
        P("ep", None),
        P("ep", None),
        P(),
        P("ep", None, "tp"),
        P("ep", None, "tp"),
        P("ep", "tp", None),
    )
    out_specs = (
        P("ep", "tp"),
        P("tp", "ep"),
        P("ep", None, "tp"),
        P("ep", None, "tp"),
        P("ep", "tp", None),
    )

    return jax.shard_map(per_device, mesh=mesh, in_specs=in_specs, out_specs=out_specs, check_vma=False)
```

```python
import functools

import jax
import jax.numpy as jnp
from jax import lax
from jax.experimental import pallas as pl
from jax.experimental.pallas import tpu as pltpu
from jax.sharding import PartitionSpec as P


F32 = jnp.float32
BF16 = jnp.bfloat16
HI = lax.Precision.HIGHEST
VMEM = pl.BlockSpec(memory_space=pltpu.VMEM)
SMEM = pl.BlockSpec(memory_space=pltpu.SMEM)


def mm(a, b, dims, precision=None):
    return lax.dot_general(a, b, (dims, ((), ())), precision=precision, preferred_element_type=F32)


NN = ((1,), (0,))
NT = ((1,), (1,))
TN = ((0,), (0,))


def iota(shape, dim):
    return lax.broadcasted_iota(jnp.int32, shape, dim)


def bits(cap):
    return cap.bit_length() - 1


def spread(experts, cap):
    rows = experts * cap
    return ((iota((rows, experts), 0) >> bits(cap)) == iota((rows, experts), 1)).astype(F32)


def dispatch_kernel(cap, tp_ref, tok_ref, og_ref, ids_ref, rw_ref, send_ref, more_ref, code_ref, gate_ref, mine_ref):
    n_tok = tok_ref.shape[0]
    experts = rw_ref.shape[0]
    share = mine_ref.shape[1]
    start = pl.multiple_of(tp_ref[0] * share, share)
    logits = mm(tok_ref[...], rw_ref[...], NT)
    ids = ids_ref[...].astype(F32).T
    lane = iota((n_tok, experts), 1).astype(F32)
    hit = lane == ids[:, 0:1]
    for k in range(1, ids.shape[1]):
        hit = hit | (lane == ids[:, k : k + 1])
    mask = hit.astype(F32)
    top = jnp.max(jnp.where(hit, logits, -jnp.inf), axis=1, keepdims=True)
    weight = jnp.where(hit, jnp.exp(jnp.where(hit, logits - top, 0.0)), 0.0)
    gate = weight / jnp.sum(weight, axis=1, keepdims=True)
    earlier = (iota((n_tok, n_tok), 1) < iota((n_tok, n_tok), 0)).astype(BF16)
    rank = mm(earlier, mask.astype(BF16), NN)
    code = mask * (rank + 1.0)
    code_ref[...] = code
    gate_ref[...] = gate
    expand = spread(experts, cap).astype(BF16)
    rows = experts * cap
    code_of = mm(expand, code.astype(BF16), NT)
    pick = code_of == ((iota((rows, n_tok), 0) & (cap - 1)) + 1).astype(F32)
    gate_of, rest = None, gate
    for _ in range(3):
        piece = rest.astype(BF16)
        rest = rest - piece.astype(F32)
        term = mm(expand, piece, NT)
        gate_of = term if gate_of is None else gate_of + term
    gate_of = jnp.sum(jnp.where(pick, gate_of, 0.0), axis=1, keepdims=True)
    mine = tok_ref[:, pl.ds(start, share)]
    mine_ref[...] = mine
    relay = send_ref.shape[1] - share
    cots = [og_ref[:, pl.ds(start, relay)]]
    cots += [og_ref[:, j + relay : j + share] for j in range(0, og_ref.shape[1], share)]
    both = mm(pick.astype(F32).astype(BF16), jnp.concatenate([mine] + cots, axis=1), NN)
    send_ref[:, :share] = both[:, :share].astype(BF16)
    send_ref[:, share:] = (both[:, share : share + relay] * gate_of).astype(BF16)
    more_ref[...] = (both[:, share + relay :] * gate_of).astype(BF16)


def joined(refs, cols):
    return jnp.concatenate([r[:, cols] for r in refs], axis=0)


def block(tp_ref, off, share):
    return pl.ds(pl.multiple_of(lax.rem(tp_ref[0] + off, 4) * share, share), share)


def forward(tp_ref, groups, share, wgu, wd, start=None):
    total = start
    for off, refs in groups:
        at = block(tp_ref, off, share)
        relay = refs[0].shape[1] - share
        terms = (
            mm(joined(refs, slice(0, share)), wgu[at, :], NN),
            mm(joined(refs, slice(share, None)), wd[:, pl.ds(at.start, relay)], NT),
        )
        total = terms if total is None else tuple(a + b for a, b in zip(total, terms))
    return total


def units(cap, both_pre, back):
    rows, ff = back.shape
    gate_pre, up_pre = both_pre[:, :ff], both_pre[:, ff:]
    glu = jnp.minimum(gate_pre, 7.0)
    linear = jnp.clip(up_pre, -7.0, 7.0)
    sig = jax.nn.sigmoid(1.702 * glu)
    act = glu * sig
    hidden = (linear + 1.0) * act
    slope = (linear + 1.0) * (sig + 1.702 * glu * sig * (1.0 - sig))
    slope = jnp.where(gate_pre < 7.0, slope, 0.0)
    up_slope = jnp.where((up_pre > -7.0) & (up_pre < 7.0), act, 0.0)
    score = jnp.sum(hidden * back, axis=1, keepdims=True)
    peers = rows // cap
    spot = ((iota((rows, 128), 0) & (cap - 1)) == iota((rows, 128), 1)).astype(F32) * score
    group = ((iota((peers, rows), 1) >> bits(cap)) == iota((peers, rows), 0)).astype(F32)
    grads = jnp.concatenate([(back * slope).astype(BF16), (back * up_slope).astype(BF16)], axis=1)
    return hidden.astype(BF16), grads, mm(group, spot, NN, HI)


def near_kernel(share, tp_ref, own, pa, pb, na, nb, more, wgu, wd, pre, bk):
    groups = ((0, (own,)), (3, (pa, pb)), (1, (na, nb)))
    relay = own.shape[1] - share
    rest = jnp.concatenate([wd[:, j + relay : j + share] for j in range(0, wd.shape[1], share)], axis=1)
    pre[...], back = forward(tp_ref, groups, share, wgu, wd)
    bk[...] = back + mm(more[...], rest, NT)


def far_kernel(cap, tp_ref, f0, f1, pre, bk, wgu, wd, hid, grads, score, b2a, b2b):
    half, share = b2a.shape
    start = (pre[...], bk[...])
    hid[...], values, score[...] = units(cap, *forward(tp_ref, ((2, (f0, f1)),), share, wgu, wd, start))
    grads[...] = values
    far = mm(values, wgu[block(tp_ref, 2, share), :], NT).astype(BF16)
    b2a[...] = far[:half]
    b2b[...] = far[half:]


def token_kernel(tp_ref, grads_ref, wgu, b1a, b3b, b0, b1b, b3a):
    share = b0.shape[1]
    half = b0.shape[0] // 2
    grads = grads_ref[...]

    def part(off):
        return mm(grads, wgu[block(tp_ref, off, share), :], NT)

    ahead = part(1)
    b1a[...] = ahead[:half]
    b1b[...] = ahead[half:].astype(BF16)
    behind = part(3)
    b3a[...] = behind[:half].astype(BF16)
    b3b[...] = behind[half:]
    b0[...] = part(0)


def total_kernel(a, b, c, d, out):
    out[...] = a[...] + b[...] + c[...] + d[...]


def onward_kernel(b1a, s1, b3b, s2, ahead, behind):
    ahead[...] = (b1a[...] + s1[...].astype(F32)).astype(BF16)
    behind[...] = (b3b[...] + s2[...].astype(F32)).astype(BF16)


def weight_kernel(share, tp_ref, own, pa, pb, na, nb, f0, f1, more, hid, grads, d_logits_ref, rw_ref,
                  gwg_ref, gwu_ref, gwd_ref, part_ref):
    ff = gwg_ref.shape[1]
    relay = own.shape[1] - share
    part_ref[...] = mm(d_logits_ref[...], rw_ref[:, block(tp_ref, 0, share)].astype(F32), NN, HI)
    rest = mm(hid[...], more[...], TN).astype(BF16)
    for j in range(gwd_ref.shape[1] // share):
        gwd_ref[:, j * share + relay : (j + 1) * share] = rest[:, j * (share - relay) : (j + 1) * (share - relay)]
    for off, refs in ((0, (own,)), (3, (pa, pb)), (1, (na, nb)), (2, (f0, f1))):
        at = block(tp_ref, off, share)
        both = mm(joined(refs, slice(0, share)), grads[...], TN).astype(BF16)
        gwg_ref[at, :] = both[:, :ff]
        gwu_ref[at, :] = both[:, ff:]
        gwd_ref[:, pl.ds(at.start, relay)] = mm(hid[...], joined(refs, slice(share, None)), TN).astype(BF16)


def router_kernel(cap, q_ref, code_ref, gate_ref, tok_ref, *refs):
    (b0, d1, d2, e1, e2), (payload_ref, d_logits_ref) = refs[:5], refs[5:]
    rows, share = b0.shape
    half = rows // 2
    for i, (near, far) in enumerate(((d2, e1), (d1, e2))):
        n = half // cap
        value = b0[i * half : (i + 1) * half] + near[...].astype(F32) + far[...].astype(F32)
        payload_ref[pl.ds(i * n, n), :, :share] = value.astype(BF16).reshape(n, cap, share)
    code, gate = code_ref[...], gate_ref[...]
    q = q_ref[...].T
    score = jnp.zeros_like(code)
    for r in range(cap):
        score = score + jnp.where(code == r + 1.0, q[r : r + 1, :], 0.0)
    d_logits = score - gate * jnp.sum(score, axis=1, keepdims=True)
    d_logits_ref[...] = d_logits
    term = mm(d_logits, tok_ref[...].astype(F32), TN, HI)
    high = term.astype(BF16)
    low = (term - high.astype(F32)).astype(BF16)
    pieces = share // 128
    for j in range(pieces):
        payload_ref[:, j, share:] = high[:, j * 128 : (j + 1) * 128]
        payload_ref[:, pieces + j, share:] = low[:, j * 128 : (j + 1) * 128]


def mark_kernel(given, out):
    out[...] = given[...]


def home_kernel(cap, home_ref, code_ref, part_ref, tok_out_ref, router_ref):
    share = part_ref.shape[1]
    code = code_ref[...]
    n_tok, experts = code.shape
    rows = experts * cap
    code_of = mm(code.astype(BF16), spread(experts, cap).astype(BF16), NT)
    pick = code_of == ((iota((n_tok, rows), 1) & (cap - 1)) + 1).astype(F32)
    flat = home_ref[...].reshape(rows, home_ref.shape[2])
    tok_out_ref[...] = (
        mm(pick.astype(F32).astype(BF16), flat[:, :share], NN) + part_ref[...]
    ).astype(BF16)
    both = jnp.sum(home_ref[:, :, share:].astype(F32), axis=0)
    pieces = share // 128
    router_ref[...] = both[:pieces] + both[pieces:]


def cost(flops, data):
    return pl.CostEstimate(flops=flops, bytes_accessed=data, transcendentals=0)


def call(body, outs, flops, scalar=True, to_hbm=0, raw=()):
    def place(i, x):
        return pltpu.with_memory_space_constraint(x, pltpu.HBM if i in raw else pltpu.VMEM)

    def run(*args):
        ins = args[1:] if scalar else args
        return pl.pallas_call(
            body,
            out_shape=[(pltpu.HBM if i < to_hbm else pltpu.VMEM)(o.shape, o.dtype) for i, o in enumerate(outs)],
            in_specs=([SMEM] if scalar else []) + [VMEM] * len(ins),
            out_specs=[VMEM] * len(outs),
            cost_estimate=cost(flops, 4 << 20),
            compiler_params=pltpu.CompilerParams(vmem_limit_bytes=24 << 20),
        )(*args[: len(args) - len(ins)], *(place(i, x) for i, x in enumerate(ins)))

    return run


def shape(dims, dtype):
    return jax.ShapeDtypeStruct(dims, dtype)


def per_device(tokens, out_grad, expert_ids, router_weight, w_gate, w_up, w_down):
    n_tok, width = tokens.shape
    experts = router_weight.shape[1]
    peers = lax.axis_size("ep")
    tp = lax.axis_size("tp")
    cap = 8
    share = width // tp
    ff = w_gate.shape[2]
    rows = peers * cap
    half = rows // 2
    me = jnp.full((1,), lax.axis_index("tp"), jnp.int32)
    unit = 2 * rows * share * ff
    router_t = router_weight.T

    def hop(value, by):
        return lax.ppermute(value, "tp", [(i, (i + by) % tp) for i in range(tp)])

    def exchange(value):
        return lax.all_to_all(value, "ep", split_axis=0, concat_axis=0, tiled=True)

    relay = share - 128
    rest = tp * (share - relay)
    send, more, code, gate, mine = call(
        functools.partial(dispatch_kernel, cap),
        [shape((rows, share + relay), BF16), shape((rows, rest), BF16), shape((n_tok, experts), F32),
         shape((n_tok, experts), F32), shape((n_tok, share), BF16)],
        unit,
        raw=(0, 1, 2, 3),
    )(me, tokens, out_grad, expert_ids.T, router_t)
    own = exchange(send.reshape(peers, cap, share + relay)).reshape(rows, share + relay)
    more = exchange(more.reshape(peers, cap, rest)).reshape(rows, rest)
    pa, nb = hop(own[:half], 1), hop(own[half:], -1)
    pb, na = hop(own[half:], 1), hop(own[:half], -1)
    f0, f1 = hop(pa, 1), hop(nb, -1)

    def load_kernel(wg, wu, wd, wgu_out, wd_out, sems):
        copies = [
            pltpu.make_async_copy(wg, wgu_out.at[:, :ff], sems.at[0]),
            pltpu.make_async_copy(wu, wgu_out.at[:, ff:], sems.at[1]),
            pltpu.make_async_copy(wd, wd_out, sems.at[2]),
        ]
        for copy in copies:
            copy.start()
        for copy in copies:
            copy.wait()

    wgu, wd = pl.pallas_call(
        load_kernel,
        out_shape=[pltpu.VMEM((width, 2 * ff), BF16), pltpu.VMEM((ff, width), BF16)],
        in_specs=[pl.BlockSpec(memory_space=pl.ANY)] * 3,
        out_specs=[VMEM] * 2,
        scratch_shapes=[pltpu.SemaphoreType.DMA((3,))],
        cost_estimate=cost(unit, 4 << 20),
        compiler_params=pltpu.CompilerParams(vmem_limit_bytes=24 << 20),
    )(*(pltpu.with_memory_space_constraint(w[0], pltpu.HBM) for w in (w_gate, w_up, w_down)))

    near = call(
        functools.partial(near_kernel, share), [shape((rows, 2 * ff), F32), shape((rows, ff), F32)], 9 * unit, raw=(0,)
    )(me, own, pa, pb, na, nb, more, wgu, wd)
    hid, grads, score, b2a, b2b = call(
        functools.partial(far_kernel, cap),
        [shape((rows, ff), BF16), shape((rows, 2 * ff), BF16), shape((peers, 128), F32)]
        + [shape((half, share), BF16)] * 2,
        5 * unit,
    )(me, f0, f1, *near, wgu, wd)
    s1, s2 = hop(b2a, 1), hop(b2b, -1)
    b1a, b3b, b0, b1b, b3a = call(
        token_kernel,
        [shape((half, share), F32)] * 2 + [shape((rows, share), F32)] + [shape((half, share), BF16)] * 2,
        6 * unit,
    )(me, grads, wgu)
    d1, d2 = hop(b1b, 1), hop(b3a, -1)
    ahead, behind = call(onward_kernel, [shape((half, share), BF16)] * 2, 1, scalar=False)(b1a, s1, b3b, s2)
    e1, e2 = hop(ahead, 1), hop(behind, -1)
    (gate,) = call(mark_kernel, [shape((n_tok, experts), F32)], 1, scalar=False)(gate)
    (score,) = call(total_kernel, [shape((peers, 128), F32)], 1, scalar=False)(
        score, hop(score, 1), hop(score, -1), hop(score, 2)
    )
    q = exchange(score.reshape(peers, 1, 128)).reshape(peers, 128)
    payload, d_logits = call(
        functools.partial(router_kernel, cap),
        [shape((peers, cap, share + 128), BF16), shape((n_tok, experts), F32)],
        unit,
        scalar=False,
    )(q, code, gate, mine, b0, d1, d2, e1, e2)
    home = exchange(payload)
    gwg, gwu, gwd, part = call(
        functools.partial(weight_kernel, share),
        [shape((width, ff), BF16), shape((width, ff), BF16), shape((ff, width), BF16), shape((n_tok, share), F32)],
        12 * unit,
        to_hbm=3,
        raw=range(12),
    )(me, own, pa, pb, na, nb, f0, f1, more, hid, grads, d_logits, router_t)
    token_grad, router = call(
        functools.partial(home_kernel, cap),
        [shape((n_tok, share), BF16), shape((share // 128, 128), F32)],
        unit,
        to_hbm=2,
        scalar=False,
    )(home, code, part)
    return (token_grad, router.reshape(share, 1), gwg[None], gwu[None], gwd[None])


def solution(mesh):
    in_specs = (
        P("ep", None),
        P("ep", None),
        P("ep", None),
        P(),
        P("ep", None, "tp"),
        P("ep", None, "tp"),
        P("ep", "tp", None),
    )
    out_specs = (
        P("ep", "tp"),
        P("tp", "ep"),
        P("ep", None, "tp"),
        P("ep", None, "tp"),
        P("ep", "tp", None),
    )

    return jax.shard_map(per_device, mesh=mesh, in_specs=in_specs, out_specs=out_specs, check_vma=False)
```

```python
import functools

import jax
import jax.numpy as jnp
from jax import lax
from jax.experimental import pallas as pl
from jax.experimental.pallas import tpu as pltpu
from jax.sharding import PartitionSpec as P


F32 = jnp.float32
BF16 = jnp.bfloat16
HI = lax.Precision.HIGHEST
VMEM = pl.BlockSpec(memory_space=pltpu.VMEM)
SMEM = pl.BlockSpec(memory_space=pltpu.SMEM)


def mm(a, b, dims, precision=None):
    return lax.dot_general(a, b, (dims, ((), ())), precision=precision, preferred_element_type=F32)


NN = ((1,), (0,))
NT = ((1,), (1,))
TN = ((0,), (0,))


def iota(shape, dim):
    return lax.broadcasted_iota(jnp.int32, shape, dim)


def bits(cap):
    return cap.bit_length() - 1


def spread(experts, cap):
    rows = experts * cap
    return ((iota((rows, experts), 0) >> bits(cap)) == iota((rows, experts), 1)).astype(F32)


def slots(cap, code, gate):
    n_tok, experts = code.shape
    rows = experts * cap
    expand = spread(experts, cap).astype(BF16)
    code_of = mm(expand, code.astype(BF16), NT)
    pick = code_of == ((iota((rows, n_tok), 0) & (cap - 1)) + 1).astype(F32)
    gate_of, rest = None, gate
    for _ in range(3):
        piece = rest.astype(BF16)
        rest = rest - piece.astype(F32)
        term = mm(expand, piece, NT)
        gate_of = term if gate_of is None else gate_of + term
    gate_of = jnp.sum(jnp.where(pick, gate_of, 0.0), axis=1, keepdims=True)
    return pick.astype(F32).astype(BF16), gate_of


def dispatch_kernel(cap, tp_ref, tok_ref, og_ref, ids_ref, rw_ref, send_ref, code_ref, gate_ref, mine_ref):
    n_tok = tok_ref.shape[0]
    experts = rw_ref.shape[0]
    share = mine_ref.shape[1]
    start = pl.multiple_of(tp_ref[0] * share, share)
    logits = mm(tok_ref[...], rw_ref[...], NT)
    ids = ids_ref[...].astype(F32).T
    lane = iota((n_tok, experts), 1).astype(F32)
    hit = lane == ids[:, 0:1]
    for k in range(1, ids.shape[1]):
        hit = hit | (lane == ids[:, k : k + 1])
    mask = hit.astype(F32)
    top = jnp.max(jnp.where(hit, logits, -jnp.inf), axis=1, keepdims=True)
    weight = jnp.where(hit, jnp.exp(jnp.where(hit, logits - top, 0.0)), 0.0)
    gate = weight / jnp.sum(weight, axis=1, keepdims=True)
    earlier = (iota((n_tok, n_tok), 1) < iota((n_tok, n_tok), 0)).astype(BF16)
    rank = mm(earlier, mask.astype(BF16), NN)
    code = mask * (rank + 1.0)
    code_ref[...] = code
    gate_ref[...] = gate
    pick, gate_of = slots(cap, code, gate)
    mine = tok_ref[:, pl.ds(start, share)]
    mine_ref[...] = mine
    relay = send_ref.shape[1] - share
    both = mm(pick, jnp.concatenate([mine, og_ref[:, pl.ds(start, relay)]], axis=1), NN)
    send_ref[:, :share] = both[:, :share].astype(BF16)
    send_ref[:, share:] = (both[:, share:] * gate_of).astype(BF16)


def direct_kernel(cap, share, code_ref, gate_ref, og_ref, more_ref):
    width = og_ref.shape[1]
    part = more_ref.shape[1] * share // width
    pick, gate_of = slots(cap, code_ref[...], gate_ref[...])
    cots = [og_ref[:, j - part : j] for j in range(share, width + 1, share)]
    more_ref[...] = (mm(pick, jnp.concatenate(cots, axis=1), NN) * gate_of).astype(BF16)


def joined(refs, cols):
    return jnp.concatenate([r[:, cols] for r in refs], axis=0)


def block(tp_ref, off, share):
    return pl.ds(pl.multiple_of(lax.rem(tp_ref[0] + off, 4) * share, share), share)


def forward(tp_ref, groups, share, wgu, wd, start=None):
    total = start
    for off, refs in groups:
        at = block(tp_ref, off, share)
        relay = refs[0].shape[1] - share
        terms = (
            mm(joined(refs, slice(0, share)), wgu[at, :], NN),
            mm(joined(refs, slice(share, None)), wd[:, pl.ds(at.start, relay)], NT),
        )
        total = terms if total is None else tuple(a + b for a, b in zip(total, terms))
    return total


def units(cap, both_pre, back):
    rows, ff = back.shape
    gate_pre, up_pre = both_pre[:, :ff], both_pre[:, ff:]
    glu = jnp.minimum(gate_pre, 7.0)
    linear = jnp.clip(up_pre, -7.0, 7.0)
    sig = jax.nn.sigmoid(1.702 * glu)
    act = glu * sig
    hidden = (linear + 1.0) * act
    slope = (linear + 1.0) * (sig + 1.702 * glu * sig * (1.0 - sig))
    slope = jnp.where(gate_pre < 7.0, slope, 0.0)
    up_slope = jnp.where((up_pre > -7.0) & (up_pre < 7.0), act, 0.0)
    score = jnp.sum(hidden * back, axis=1, keepdims=True)
    peers = rows // cap
    spot = ((iota((rows, 128), 0) & (cap - 1)) == iota((rows, 128), 1)).astype(F32) * score
    group = ((iota((peers, rows), 1) >> bits(cap)) == iota((peers, rows), 0)).astype(F32)
    grads = jnp.concatenate([(back * slope).astype(BF16), (back * up_slope).astype(BF16)], axis=1)
    return hidden.astype(BF16), grads, mm(group, spot, NN, HI)


def near_kernel(share, tp_ref, own, pa, pb, na, nb, wgu, wd, pre, bk):
    groups = ((0, (own,)), (3, (pa, pb)), (1, (na, nb)))
    pre[...], bk[...] = forward(tp_ref, groups, share, wgu, wd)


def far_kernel(cap, tp_ref, f0, f1, more, pre, bk, wgu, wd, hid, grads, score, b2a, b2b):
    half, share = b2a.shape
    relay = f0.shape[1] - share
    rest = jnp.concatenate([wd[:, j + relay : j + share] for j in range(0, wd.shape[1], share)], axis=1)
    start = (pre[...], bk[...] + mm(more[...], rest, NT))
    hid[...], values, score[...] = units(cap, *forward(tp_ref, ((2, (f0, f1)),), share, wgu, wd, start))
    grads[...] = values
    far = mm(values, wgu[block(tp_ref, 2, share), :], NT).astype(BF16)
    b2a[...] = far[:half]
    b2b[...] = far[half:]


def token_kernel(tp_ref, grads_ref, wgu, b1a, b3b, b0, b1b, b3a):
    share = b0.shape[1]
    half = b0.shape[0] // 2
    grads = grads_ref[...]

    def part(off):
        return mm(grads, wgu[block(tp_ref, off, share), :], NT)

    ahead = part(1)
    b1a[...] = ahead[:half]
    b1b[...] = ahead[half:].astype(BF16)
    behind = part(3)
    b3a[...] = behind[:half].astype(BF16)
    b3b[...] = behind[half:]
    b0[...] = part(0)


def total_kernel(a, b, c, d, out):
    out[...] = a[...] + b[...] + c[...] + d[...]


def onward_kernel(b1a, s1, b3b, s2, ahead, behind):
    ahead[...] = (b1a[...] + s1[...].astype(F32)).astype(BF16)
    behind[...] = (b3b[...] + s2[...].astype(F32)).astype(BF16)


def weight_kernel(share, tp_ref, own, pa, pb, na, nb, f0, f1, more, hid, grads, d_logits_ref, rw_ref,
                  gwg_ref, gwu_ref, gwd_ref, part_ref):
    ff = gwg_ref.shape[1]
    relay = own.shape[1] - share
    part_ref[...] = mm(d_logits_ref[...], rw_ref[:, block(tp_ref, 0, share)].astype(F32), NN, HI)
    rest = mm(hid[...], more[...], TN).astype(BF16)
    for j in range(gwd_ref.shape[1] // share):
        gwd_ref[:, j * share + relay : (j + 1) * share] = rest[:, j * (share - relay) : (j + 1) * (share - relay)]
    for off, refs in ((0, (own,)), (3, (pa, pb)), (1, (na, nb)), (2, (f0, f1))):
        at = block(tp_ref, off, share)
        both = mm(joined(refs, slice(0, share)), grads[...], TN).astype(BF16)
        gwg_ref[at, :] = both[:, :ff]
        gwu_ref[at, :] = both[:, ff:]
        gwd_ref[:, pl.ds(at.start, relay)] = mm(hid[...], joined(refs, slice(share, None)), TN).astype(BF16)


def router_kernel(cap, q_ref, code_ref, gate_ref, tok_ref, *refs):
    (b0, d1, d2, e1, e2), (payload_ref, d_logits_ref) = refs[:5], refs[5:]
    rows, share = b0.shape
    half = rows // 2
    for i, (near, far) in enumerate(((d2, e1), (d1, e2))):
        n = half // cap
        value = b0[i * half : (i + 1) * half] + near[...].astype(F32) + far[...].astype(F32)
        payload_ref[pl.ds(i * n, n), :, :share] = value.astype(BF16).reshape(n, cap, share)
    code, gate = code_ref[...], gate_ref[...]
    q = q_ref[...].T
    score = jnp.zeros_like(code)
    for r in range(cap):
        score = score + jnp.where(code == r + 1.0, q[r : r + 1, :], 0.0)
    d_logits = score - gate * jnp.sum(score, axis=1, keepdims=True)
    d_logits_ref[...] = d_logits
    term = mm(d_logits, tok_ref[...].astype(F32), TN, HI)
    high = term.astype(BF16)
    low = (term - high.astype(F32)).astype(BF16)
    pieces = share // 128
    for j in range(pieces):
        payload_ref[:, j, share:] = high[:, j * 128 : (j + 1) * 128]
        payload_ref[:, pieces + j, share:] = low[:, j * 128 : (j + 1) * 128]


def mark_kernel(given, out):
    out[...] = given[...]


def home_kernel(cap, home_ref, code_ref, part_ref, tok_out_ref, router_ref):
    share = part_ref.shape[1]
    code = code_ref[...]
    n_tok, experts = code.shape
    rows = experts * cap
    code_of = mm(code.astype(BF16), spread(experts, cap).astype(BF16), NT)
    pick = code_of == ((iota((n_tok, rows), 1) & (cap - 1)) + 1).astype(F32)
    flat = home_ref[...].reshape(rows, home_ref.shape[2])
    tok_out_ref[...] = (
        mm(pick.astype(F32).astype(BF16), flat[:, :share], NN) + part_ref[...]
    ).astype(BF16)
    both = jnp.sum(home_ref[:, :, share:].astype(F32), axis=0)
    pieces = share // 128
    router_ref[...] = both[:pieces] + both[pieces:]


def cost(flops, data):
    return pl.CostEstimate(flops=flops, bytes_accessed=data, transcendentals=0)


def call(body, outs, flops, scalar=True, to_hbm=0, raw=()):
    def place(i, x):
        return pltpu.with_memory_space_constraint(x, pltpu.HBM if i in raw else pltpu.VMEM)

    def run(*args):
        ins = args[1:] if scalar else args
        return pl.pallas_call(
            body,
            out_shape=[(pltpu.HBM if i < to_hbm else pltpu.VMEM)(o.shape, o.dtype) for i, o in enumerate(outs)],
            in_specs=([SMEM] if scalar else []) + [VMEM] * len(ins),
            out_specs=[VMEM] * len(outs),
            cost_estimate=cost(flops, 4 << 20),
            compiler_params=pltpu.CompilerParams(vmem_limit_bytes=24 << 20),
        )(*args[: len(args) - len(ins)], *(place(i, x) for i, x in enumerate(ins)))

    return run


def shape(dims, dtype):
    return jax.ShapeDtypeStruct(dims, dtype)


def per_device(tokens, out_grad, expert_ids, router_weight, w_gate, w_up, w_down):
    n_tok, width = tokens.shape
    experts = router_weight.shape[1]
    peers = lax.axis_size("ep")
    tp = lax.axis_size("tp")
    cap = 8
    share = width // tp
    ff = w_gate.shape[2]
    rows = peers * cap
    half = rows // 2
    me = jnp.full((1,), lax.axis_index("tp"), jnp.int32)
    unit = 2 * rows * share * ff
    router_t = router_weight.T

    def hop(value, by):
        return lax.ppermute(value, "tp", [(i, (i + by) % tp) for i in range(tp)])

    def exchange(value):
        return lax.all_to_all(value, "ep", split_axis=0, concat_axis=0, tiled=True)

    relay = share - 128
    rest = tp * (share - relay)
    send, code, gate, mine = call(
        functools.partial(dispatch_kernel, cap),
        [shape((rows, share + relay), BF16), shape((n_tok, experts), F32),
         shape((n_tok, experts), F32), shape((n_tok, share), BF16)],
        unit,
        raw=(0, 1, 2, 3),
    )(me, tokens, out_grad, expert_ids.T, router_t)
    (more,) = call(
        functools.partial(direct_kernel, cap, share), [shape((rows, rest), BF16)], unit, scalar=False, raw=(2,)
    )(code, gate, out_grad)
    own = exchange(send.reshape(peers, cap, share + relay)).reshape(rows, share + relay)
    more = exchange(more.reshape(peers, cap, rest)).reshape(rows, rest)
    pa, nb = hop(own[:half], 1), hop(own[half:], -1)
    pb, na = hop(own[half:], 1), hop(own[:half], -1)
    f0, f1 = hop(pa, 1), hop(nb, -1)

    def load(turn):
        def load_kernel(wg, wu, wd, wgu_out, wd_out, sems):
            copies = [
                pltpu.make_async_copy(wg, wgu_out.at[:, :ff], sems.at[0]),
                pltpu.make_async_copy(wu, wgu_out.at[:, ff:], sems.at[1]),
                pltpu.make_async_copy(wd, wd_out, sems.at[2]),
            ]
            for copy in copies if turn else copies[::-1]:
                copy.start()
            for copy in copies:
                copy.wait()

        return pl.pallas_call(
            load_kernel,
            out_shape=[pltpu.VMEM((width, 2 * ff), BF16), pltpu.VMEM((ff, width), BF16)],
            in_specs=[pl.BlockSpec(memory_space=pl.ANY)] * 3,
            out_specs=[VMEM] * 2,
            scratch_shapes=[pltpu.SemaphoreType.DMA((3,))],
            cost_estimate=cost(unit, 4 << 20),
            compiler_params=pltpu.CompilerParams(vmem_limit_bytes=24 << 20),
        )(*(pltpu.with_memory_space_constraint(w[0], pltpu.HBM) for w in (w_gate, w_up, w_down)))

    wgu, wd = load(1)
    near = call(
        functools.partial(near_kernel, share),
        [shape((rows, 2 * ff), F32), shape((rows, ff), F32)],
        9 * unit,
        raw=(0, 2, 3),
    )(me, own, pa, pb, na, nb, *load(0))
    hid, grads, score, b2a, b2b = call(
        functools.partial(far_kernel, cap),
        [shape((rows, ff), BF16), shape((rows, 2 * ff), BF16), shape((peers, 128), F32)]
        + [shape((half, share), BF16)] * 2,
        5 * unit,
        raw=(2,),
    )(me, f0, f1, more, *near, wgu, wd)
    s1, s2 = hop(b2a, 1), hop(b2b, -1)
    b1a, b3b, b0, b1b, b3a = call(
        token_kernel,
        [shape((half, share), F32)] * 2 + [shape((rows, share), F32)] + [shape((half, share), BF16)] * 2,
        6 * unit,
    )(me, grads, wgu)
    d1, d2 = hop(b1b, 1), hop(b3a, -1)
    ahead, behind = call(onward_kernel, [shape((half, share), BF16)] * 2, 1, scalar=False)(b1a, s1, b3b, s2)
    e1, e2 = hop(ahead, 1), hop(behind, -1)
    (gate,) = call(mark_kernel, [shape((n_tok, experts), F32)], 1, scalar=False)(gate)
    (score,) = call(total_kernel, [shape((peers, 128), F32)], 1, scalar=False)(
        score, hop(score, 1), hop(score, -1), hop(score, 2)
    )
    q = exchange(score.reshape(peers, 1, 128)).reshape(peers, 128)
    payload, d_logits = call(
        functools.partial(router_kernel, cap),
        [shape((peers, cap, share + 128), BF16), shape((n_tok, experts), F32)],
        unit,
        scalar=False,
    )(q, code, gate, mine, b0, d1, d2, e1, e2)
    home = exchange(payload)
    gwg, gwu, gwd, part = call(
        functools.partial(weight_kernel, share),
        [shape((width, ff), BF16), shape((width, ff), BF16), shape((ff, width), BF16), shape((n_tok, share), F32)],
        12 * unit,
        to_hbm=3,
        raw=range(12),
    )(me, own, pa, pb, na, nb, f0, f1, more, hid, grads, d_logits, router_t)
    token_grad, router = call(
        functools.partial(home_kernel, cap),
        [shape((n_tok, share), BF16), shape((share // 128, 128), F32)],
        unit,
        to_hbm=2,
        scalar=False,
    )(home, code, part)
    return (token_grad, router.reshape(share, 1), gwg[None], gwu[None], gwd[None])


def solution(mesh):
    in_specs = (
        P("ep", None),
        P("ep", None),
        P("ep", None),
        P(),
        P("ep", None, "tp"),
        P("ep", None, "tp"),
        P("ep", "tp", None),
    )
    out_specs = (
        P("ep", "tp"),
        P("tp", "ep"),
        P("ep", None, "tp"),
        P("ep", None, "tp"),
        P("ep", "tp", None),
    )

    return jax.shard_map(per_device, mesh=mesh, in_specs=in_specs, out_specs=out_specs, check_vma=False)
```

```python
import functools

import jax
import jax.numpy as jnp
from jax import lax
from jax.experimental import pallas as pl
from jax.experimental.pallas import tpu as pltpu
from jax.sharding import PartitionSpec as P


F32 = jnp.float32
BF16 = jnp.bfloat16
HI = lax.Precision.HIGHEST
VMEM = pl.BlockSpec(memory_space=pltpu.VMEM)
SMEM = pl.BlockSpec(memory_space=pltpu.SMEM)


def mm(a, b, dims, precision=None):
    return lax.dot_general(a, b, (dims, ((), ())), precision=precision, preferred_element_type=F32)


NN = ((1,), (0,))
NT = ((1,), (1,))
TN = ((0,), (0,))


def iota(shape, dim):
    return lax.broadcasted_iota(jnp.int32, shape, dim)


def bits(cap):
    return cap.bit_length() - 1


def spread(experts, cap):
    rows = experts * cap
    return ((iota((rows, experts), 0) >> bits(cap)) == iota((rows, experts), 1)).astype(F32)


def slots(cap, code, gate):
    n_tok, experts = code.shape
    rows = experts * cap
    expand = spread(experts, cap).astype(BF16)
    code_of = mm(expand, code.astype(BF16), NT)
    pick = code_of == ((iota((rows, n_tok), 0) & (cap - 1)) + 1).astype(F32)
    gate_of, rest = None, gate
    for _ in range(3):
        piece = rest.astype(BF16)
        rest = rest - piece.astype(F32)
        term = mm(expand, piece, NT)
        gate_of = term if gate_of is None else gate_of + term
    gate_of = jnp.sum(jnp.where(pick, gate_of, 0.0), axis=1, keepdims=True)
    return pick.astype(F32).astype(BF16), gate_of


def dispatch_kernel(cap, tp_ref, tok_ref, og_ref, ids_ref, rw_ref, send_ref, code_ref, gate_ref, mine_ref):
    n_tok = tok_ref.shape[0]
    experts = rw_ref.shape[0]
    share = mine_ref.shape[1]
    start = pl.multiple_of(tp_ref[0] * share, share)
    logits = mm(tok_ref[...], rw_ref[...], NT)
    ids = ids_ref[...].astype(F32).T
    lane = iota((n_tok, experts), 1).astype(F32)
    hit = lane == ids[:, 0:1]
    for k in range(1, ids.shape[1]):
        hit = hit | (lane == ids[:, k : k + 1])
    mask = hit.astype(F32)
    top = jnp.max(jnp.where(hit, logits, -jnp.inf), axis=1, keepdims=True)
    weight = jnp.where(hit, jnp.exp(jnp.where(hit, logits - top, 0.0)), 0.0)
    gate = weight / jnp.sum(weight, axis=1, keepdims=True)
    earlier = (iota((n_tok, n_tok), 1) < iota((n_tok, n_tok), 0)).astype(BF16)
    rank = mm(earlier, mask.astype(BF16), NN)
    code = mask * (rank + 1.0)
    code_ref[...] = code
    gate_ref[...] = gate
    pick, gate_of = slots(cap, code, gate)
    mine = tok_ref[:, pl.ds(start, share)]
    mine_ref[...] = mine
    relay = send_ref.shape[1] - share
    both = mm(pick, jnp.concatenate([mine, og_ref[:, pl.ds(start, relay)]], axis=1), NN)
    send_ref[:, :share] = both[:, :share].astype(BF16)
    send_ref[:, share:] = (both[:, share:] * gate_of).astype(BF16)


def direct_kernel(cap, share, code_ref, gate_ref, og_ref, more_ref):
    width = og_ref.shape[1]
    part = more_ref.shape[1] * share // width
    pick, gate_of = slots(cap, code_ref[...], gate_ref[...])
    cots = [og_ref[:, j - part : j] for j in range(share, width + 1, share)]
    more_ref[...] = (mm(pick, jnp.concatenate(cots, axis=1), NN) * gate_of).astype(BF16)


def joined(refs, cols):
    return jnp.concatenate([r[:, cols] for r in refs], axis=0)


def block(tp_ref, off, share):
    return pl.ds(pl.multiple_of(lax.rem(tp_ref[0] + off, 4) * share, share), share)


def forward(tp_ref, groups, share, wgu, wd, start=None):
    total = start
    for off, refs in groups:
        at = block(tp_ref, off, share)
        relay = refs[0].shape[1] - share
        terms = (
            mm(joined(refs, slice(0, share)), wgu[at, :], NN),
            mm(joined(refs, slice(share, None)), wd[:, pl.ds(at.start, relay)], NT),
        )
        total = terms if total is None else tuple(a + b for a, b in zip(total, terms))
    return total


def units(cap, both_pre, back):
    rows, ff = back.shape
    gate_pre, up_pre = both_pre[:, :ff], both_pre[:, ff:]
    glu = jnp.minimum(gate_pre, 7.0)
    linear = jnp.clip(up_pre, -7.0, 7.0)
    sig = jax.nn.sigmoid(1.702 * glu)
    act = glu * sig
    hidden = (linear + 1.0) * act
    slope = (linear + 1.0) * (sig + 1.702 * glu * sig * (1.0 - sig))
    slope = jnp.where(gate_pre < 7.0, slope, 0.0)
    up_slope = jnp.where((up_pre > -7.0) & (up_pre < 7.0), act, 0.0)
    score = jnp.sum(hidden * back, axis=1, keepdims=True)
    peers = rows // cap
    spot = ((iota((rows, 128), 0) & (cap - 1)) == iota((rows, 128), 1)).astype(F32) * score
    group = ((iota((peers, rows), 1) >> bits(cap)) == iota((peers, rows), 0)).astype(F32)
    grads = jnp.concatenate([(back * slope).astype(BF16), (back * up_slope).astype(BF16)], axis=1)
    return hidden.astype(BF16), grads, mm(group, spot, NN, HI)


def near_kernel(share, tp_ref, own, pa, pb, na, nb, wgu, wd, pre, bk):
    groups = ((0, (own,)), (3, (pa, pb)), (1, (na, nb)))
    pre[...], bk[...] = forward(tp_ref, groups, share, wgu, wd)


def far_kernel(cap, tp_ref, f0, f1, more, pre, bk, wgu, wd, hid, grads, score, b2a, b2b):
    half, share = b2a.shape
    relay = f0.shape[1] - share
    rest = jnp.concatenate([wd[:, j + relay : j + share] for j in range(0, wd.shape[1], share)], axis=1)
    start = (pre[...], bk[...] + mm(more[...], rest, NT))
    hid[...], values, score[...] = units(cap, *forward(tp_ref, ((2, (f0, f1)),), share, wgu, wd, start))
    grads[...] = values
    far = mm(values, wgu[block(tp_ref, 2, share), :], NT).astype(BF16)
    b2a[...] = far[:half]
    b2b[...] = far[half:]


def token_kernel(tp_ref, grads_ref, wgu, b1a, b3b, b0, b1b, b3a):
    share = b0.shape[1]
    half = b0.shape[0] // 2
    grads = grads_ref[...]

    def part(off):
        return mm(grads, wgu[block(tp_ref, off, share), :], NT)

    ahead = part(1)
    b1a[...] = ahead[:half]
    b1b[...] = ahead[half:].astype(BF16)
    behind = part(3)
    b3a[...] = behind[:half].astype(BF16)
    b3b[...] = behind[half:]
    b0[...] = part(0)


def total_kernel(a, b, c, d, out):
    out[...] = a[...] + b[...] + c[...] + d[...]


def onward_kernel(b1a, s1, b3b, s2, ahead, behind):
    ahead[...] = (b1a[...] + s1[...].astype(F32)).astype(BF16)
    behind[...] = (b3b[...] + s2[...].astype(F32)).astype(BF16)


def weight_kernel(share, tp_ref, own, pa, pb, na, nb, f0, f1, more, hid, grads, d_logits_ref, rw_ref,
                  gwg_ref, gwu_ref, gwd_ref, part_ref):
    ff = gwg_ref.shape[1]
    relay = own.shape[1] - share
    part_ref[...] = mm(d_logits_ref[...], rw_ref[:, block(tp_ref, 0, share)].astype(F32), NN, HI)
    rest = mm(hid[...], more[...], TN).astype(BF16)
    for j in range(gwd_ref.shape[1] // share):
        gwd_ref[:, j * share + relay : (j + 1) * share] = rest[:, j * (share - relay) : (j + 1) * (share - relay)]
    for off, refs in ((0, (own,)), (3, (pa, pb)), (1, (na, nb)), (2, (f0, f1))):
        at = block(tp_ref, off, share)
        both = mm(joined(refs, slice(0, share)), grads[...], TN).astype(BF16)
        gwg_ref[at, :] = both[:, :ff]
        gwu_ref[at, :] = both[:, ff:]
        gwd_ref[:, pl.ds(at.start, relay)] = mm(hid[...], joined(refs, slice(share, None)), TN).astype(BF16)


def router_kernel(cap, q_ref, code_ref, gate_ref, tok_ref, term_ref, d_logits_ref):
    code, gate = code_ref[...], gate_ref[...]
    q = q_ref[...].T
    score = jnp.zeros_like(code)
    for r in range(cap):
        score = score + jnp.where(code == r + 1.0, q[r : r + 1, :], 0.0)
    d_logits = score - gate * jnp.sum(score, axis=1, keepdims=True)
    d_logits_ref[...] = d_logits
    term = mm(d_logits, tok_ref[...].astype(F32), TN, HI)
    high = term.astype(BF16)
    low = (term - high.astype(F32)).astype(BF16)
    pieces = term.shape[1] // 128
    for j in range(pieces):
        term_ref[:, j, :] = high[:, j * 128 : (j + 1) * 128]
        term_ref[:, pieces + j, :] = low[:, j * 128 : (j + 1) * 128]


def pack_kernel(cap, b0, d1, d2, e1, e2, term_ref, payload_ref):
    rows, share = b0.shape
    half = rows // 2
    for i, (near, far) in enumerate(((d2, e1), (d1, e2))):
        n = half // cap
        value = b0[i * half : (i + 1) * half] + near[...].astype(F32) + far[...].astype(F32)
        payload_ref[pl.ds(i * n, n), :, :share] = value.astype(BF16).reshape(n, cap, share)
    payload_ref[:, :, share:] = term_ref[...]


def mark_kernel(given, out):
    out[...] = given[...]


def home_kernel(cap, home_ref, code_ref, part_ref, tok_out_ref, router_ref):
    share = part_ref.shape[1]
    code = code_ref[...]
    n_tok, experts = code.shape
    rows = experts * cap
    code_of = mm(code.astype(BF16), spread(experts, cap).astype(BF16), NT)
    pick = code_of == ((iota((n_tok, rows), 1) & (cap - 1)) + 1).astype(F32)
    flat = home_ref[...].reshape(rows, home_ref.shape[2])
    tok_out_ref[...] = (
        mm(pick.astype(F32).astype(BF16), flat[:, :share], NN) + part_ref[...]
    ).astype(BF16)
    both = jnp.sum(home_ref[:, :, share:].astype(F32), axis=0)
    pieces = share // 128
    router_ref[...] = both[:pieces] + both[pieces:]


def cost(flops, data):
    return pl.CostEstimate(flops=flops, bytes_accessed=data, transcendentals=0)


def call(body, outs, flops, scalar=True, to_hbm=0, raw=()):
    def place(i, x):
        return pltpu.with_memory_space_constraint(x, pltpu.HBM if i in raw else pltpu.VMEM)

    def run(*args):
        ins = args[1:] if scalar else args
        return pl.pallas_call(
            body,
            out_shape=[(pltpu.HBM if i < to_hbm else pltpu.VMEM)(o.shape, o.dtype) for i, o in enumerate(outs)],
            in_specs=([SMEM] if scalar else []) + [VMEM] * len(ins),
            out_specs=[VMEM] * len(outs),
            cost_estimate=cost(flops, 4 << 20),
            compiler_params=pltpu.CompilerParams(vmem_limit_bytes=24 << 20),
        )(*args[: len(args) - len(ins)], *(place(i, x) for i, x in enumerate(ins)))

    return run


def shape(dims, dtype):
    return jax.ShapeDtypeStruct(dims, dtype)


def per_device(tokens, out_grad, expert_ids, router_weight, w_gate, w_up, w_down):
    n_tok, width = tokens.shape
    experts = router_weight.shape[1]
    peers = lax.axis_size("ep")
    tp = lax.axis_size("tp")
    cap = 8
    share = width // tp
    ff = w_gate.shape[2]
    rows = peers * cap
    half = rows // 2
    me = jnp.full((1,), lax.axis_index("tp"), jnp.int32)
    unit = 2 * rows * share * ff
    router_t = router_weight.T

    def hop(value, by):
        return lax.ppermute(value, "tp", [(i, (i + by) % tp) for i in range(tp)])

    def exchange(value):
        return lax.all_to_all(value, "ep", split_axis=0, concat_axis=0, tiled=True)

    relay = share - 128
    rest = tp * (share - relay)
    send, code, gate, mine = call(
        functools.partial(dispatch_kernel, cap),
        [shape((rows, share + relay), BF16), shape((n_tok, experts), F32),
         shape((n_tok, experts), F32), shape((n_tok, share), BF16)],
        unit,
        raw=(0, 1, 2, 3),
    )(me, tokens, out_grad, expert_ids.T, router_t)
    (more,) = call(
        functools.partial(direct_kernel, cap, share), [shape((rows, rest), BF16)], unit, scalar=False, raw=(2,)
    )(code, gate, out_grad)
    own = exchange(send.reshape(peers, cap, share + relay)).reshape(rows, share + relay)
    more = exchange(more.reshape(peers, cap, rest)).reshape(rows, rest)
    pa, nb = hop(own[:half], 1), hop(own[half:], -1)
    pb, na = hop(own[half:], 1), hop(own[:half], -1)
    f0, f1 = hop(pa, 1), hop(nb, -1)

    def load(*others):
        arrays = [w_gate[0], w_up[0], w_down[0], *others]

        def load_kernel(*refs):
            (wg, wu, *sources), (wgu_out, *targets), sems = refs[: len(arrays)], refs[len(arrays) : -1], refs[-1]
            copies = [
                pltpu.make_async_copy(wg, wgu_out.at[:, :ff], sems.at[0]),
                pltpu.make_async_copy(wu, wgu_out.at[:, ff:], sems.at[1]),
            ]
            for i, (source, target) in enumerate(zip(sources, targets)):
                copies.append(pltpu.make_async_copy(source, target, sems.at[2 + i]))
            for copy in copies:
                copy.start()
            for copy in copies:
                copy.wait()

        return pl.pallas_call(
            load_kernel,
            out_shape=[pltpu.VMEM((width, 2 * ff), BF16)] + [pltpu.VMEM(a.shape, a.dtype) for a in arrays[2:]],
            in_specs=[pl.BlockSpec(memory_space=pl.ANY)] * len(arrays),
            out_specs=[VMEM] * (len(arrays) - 1),
            scratch_shapes=[pltpu.SemaphoreType.DMA((len(arrays),))],
            cost_estimate=cost(unit, 4 << 20),
            compiler_params=pltpu.CompilerParams(vmem_limit_bytes=24 << 20),
        )(*(pltpu.with_memory_space_constraint(a, pltpu.HBM) for a in arrays))

    wgu, wd, more_near = load(more)
    near = call(
        functools.partial(near_kernel, share),
        [shape((rows, 2 * ff), F32), shape((rows, ff), F32)],
        9 * unit,
        raw=(0, 2, 3),
    )(me, own, pa, pb, na, nb, *load())
    hid, grads, score, b2a, b2b = call(
        functools.partial(far_kernel, cap),
        [shape((rows, ff), BF16), shape((rows, 2 * ff), BF16), shape((peers, 128), F32)]
        + [shape((half, share), BF16)] * 2,
        5 * unit,
    )(me, f0, f1, more_near, *near, wgu, wd)
    s1, s2 = hop(b2a, 1), hop(b2b, -1)
    b1a, b3b, b0, b1b, b3a = call(
        token_kernel,
        [shape((half, share), F32)] * 2 + [shape((rows, share), F32)] + [shape((half, share), BF16)] * 2,
        6 * unit,
    )(me, grads, wgu)
    d1, d2 = hop(b1b, 1), hop(b3a, -1)
    ahead, behind = call(onward_kernel, [shape((half, share), BF16)] * 2, 1, scalar=False)(b1a, s1, b3b, s2)
    e1, e2 = hop(ahead, 1), hop(behind, -1)
    (gate,) = call(mark_kernel, [shape((n_tok, experts), F32)], 1, scalar=False)(gate)
    (score,) = call(total_kernel, [shape((peers, 128), F32)], 1, scalar=False)(
        score, hop(score, 1), hop(score, -1), hop(score, 2)
    )
    q = exchange(score.reshape(peers, 1, 128)).reshape(peers, 128)
    term, d_logits = call(
        functools.partial(router_kernel, cap),
        [shape((peers, cap, 128), BF16), shape((n_tok, experts), F32)],
        unit,
        scalar=False,
    )(q, code, gate, mine)
    (payload,) = call(
        functools.partial(pack_kernel, cap), [shape((peers, cap, share + 128), BF16)], unit, scalar=False
    )(b0, d1, d2, e1, e2, term)
    home = exchange(payload)
    gwg, gwu, gwd, part = call(
        functools.partial(weight_kernel, share),
        [shape((width, ff), BF16), shape((width, ff), BF16), shape((ff, width), BF16), shape((n_tok, share), F32)],
        12 * unit,
        to_hbm=3,
        raw=range(12),
    )(me, own, pa, pb, na, nb, f0, f1, more, hid, grads, d_logits, router_t)
    token_grad, router = call(
        functools.partial(home_kernel, cap),
        [shape((n_tok, share), BF16), shape((share // 128, 128), F32)],
        unit,
        to_hbm=2,
        scalar=False,
    )(home, code, part)
    return (token_grad, router.reshape(share, 1), gwg[None], gwu[None], gwd[None])


def solution(mesh):
    in_specs = (
        P("ep", None),
        P("ep", None),
        P("ep", None),
        P(),
        P("ep", None, "tp"),
        P("ep", None, "tp"),
        P("ep", "tp", None),
    )
    out_specs = (
        P("ep", "tp"),
        P("tp", "ep"),
        P("ep", None, "tp"),
        P("ep", None, "tp"),
        P("ep", "tp", None),
    )

    return jax.shard_map(per_device, mesh=mesh, in_specs=in_specs, out_specs=out_specs, check_vma=False)
```
